512 devices in a mesh: ep: 32 (over z, core), tp: 16 (over y, x).
Axes of the slice: x: 4, y: 4, z: 16, core: 2. Of those that a mesh axis runs over, the one named last changes fastest.
Arguments:
- queries: bfloat16 [8192, 2048], P('ep', 'tp'), may hold values from -6 to 6
- keys: bfloat16 [8192, 2048], P('ep', 'tp'), may hold values from -6 to 6
- values: bfloat16 [8192, 2048], P('ep', 'tp'), may hold values from -6 to 6
- gates: bfloat16 [8192, 2048], P('ep', 'tp'), may hold values from -6 to 6
- log_decay: float32 [8192, 16], P('ep', 'tp'), may hold values from -2 to 0
- out_weight: bfloat16 [2048, 2048], P(None, 'tp'), may hold values from -0.125 to 0.125
- moe_rows: bfloat16 [8192, 2048], P('ep'), may hold values from -140 to 140
- moe_gain: bfloat16 [2048], replicated, may hold values from 0.099609375 to 1.8984375
- routes: int32 [8192, 2], P('ep'), may hold values from 0 to 31, as said below
- route_weights: float32 [8192, 2], P('ep'), may hold values from 0.1 to 1
- gate_proj: bfloat16 [32, 2048, 4096], P('ep', None, 'tp'), may hold values from -0.125 to 0.125
- up_proj: bfloat16 [32, 2048, 4096], P('ep', None, 'tp'), may hold values from -0.125 to 0.125
- down_proj: bfloat16 [32, 4096, 2048], P('ep', None, 'tp'), may hold values from -0.09375 to 0.09375
Outputs:
- mixer_out: bfloat16 [8192, 2048], P('ep', 'tp')
- moe_out: bfloat16 [8192, 2048], P('ep', 'tp')
The draws below stay inside these ranges and needn't reach their ends.
Inputs may be any that keep to these rules, and one draw needn't show every extreme that they name: `routes`: each row names two different experts of one group of 8 consecutive experts; in each aligned block of 256 rows every expert is named by exactly 16 rows.
All inputs are finite; a program needn't handle non-finite values.
Results may differ from the reference program's by a relative error of at most 0.011.
Values may be sent and summed in bfloat16 or wider, within the bound.
A program may use at most 64 MiB of HBM per device.

```python
import math
import jax
import jax.numpy as jnp
from jax import lax

D = 2048
RETENTION_HEADS = 16
HEAD_DIM = 128
FF = 4096
EXP_GROUP = 8
BLOCK = 128
ROWS_MIX = 256
ROWS_MOE = 256
MIXER_TOKENS = 8192
TOKENS_MOE = 8192
EXPERTS = 32
GROUPS = 4


def draw_log_decay(key, part):
    k_fast = jax.random.fold_in(key, 11)
    k_rate = jax.random.fold_in(key, 12)
    k_slow = jax.random.fold_in(key, 13)
    k_block = jax.random.fold_in(key, 14)
    k_rough = jax.random.fold_in(key, 15)
    location_random_key = jax.random.fold_in(key, 16)
    spike_random_key = jax.random.fold_in(key, 17)
    fast_share = 0.5
    is_fast = jax.random.uniform(k_fast, (RETENTION_HEADS,)) < fast_share
    fast_rate = jax.random.uniform(k_rate, (RETENTION_HEADS,), minval=2.5, maxval=4.0) / BLOCK
    slow_rate = jax.random.uniform(k_slow, (RETENTION_HEADS,), minval=0.1, maxval=0.35) / MIXER_TOKENS
    baseline_decay_rate = jnp.where(is_fast, fast_rate, slow_rate)
    span_count = MIXER_TOKENS // ROWS_MIX
    extent_multiplier = jnp.exp(jax.random.uniform(k_block, (span_count, RETENTION_HEADS), minval=-math.log(2.0), maxval=math.log(2.0)))
    extent_multiplier = jnp.repeat(extent_multiplier, ROWS_MIX, axis=0)
    jitter_multiplier = jnp.exp(jax.random.uniform(k_rough, (MIXER_TOKENS, RETENTION_HEADS), minval=-0.7, maxval=0.7))
    spike_locations = jax.random.randint(location_random_key, (2, RETENTION_HEADS), 0, MIXER_TOKENS)
    spike_strength = jnp.log(jax.random.uniform(spike_random_key, (2, RETENTION_HEADS), minval=0.5, maxval=0.8))
    token_place = jnp.arange(MIXER_TOKENS, dtype=jnp.int32)[None, :, None]
    decay_spikes = jnp.sum(jnp.where(token_place == spike_locations[:, None, :], spike_strength[:, None, :], 0.0), axis=0)
    return (decay_spikes - baseline_decay_rate[None, :] * extent_multiplier * jitter_multiplier).astype(jnp.float32)


def draw_moe_rows(key, part):
    k_base = jax.random.fold_in(key, 21)
    k_column = jax.random.fold_in(key, 22)
    base = jax.random.truncated_normal(k_base, -4.0, 4.0, (TOKENS_MOE, D))
    column_scale = jnp.exp(jax.random.uniform(k_column, (D,), minval=0.0, maxval=math.log(10.0)))
    result = base * column_scale[None, :]
    return result.astype(jnp.bfloat16)


def draw_routes(key, part):
    k_perm = jax.random.fold_in(key, 31)
    k_first = jax.random.fold_in(key, 32)
    k_second = jax.random.fold_in(key, 33)
    span_count = TOKENS_MOE // ROWS_MOE
    orders = jax.vmap(lambda single: jax.random.permutation(single, ROWS_MOE))(jax.random.split(k_perm, span_count))
    ranked = jnp.argsort(orders, axis=1, stable=True).astype(jnp.int32)
    group_id = ranked % GROUPS
    local_rank = ranked // GROUPS
    first_offset = jax.random.randint(k_first, (span_count, GROUPS), 0, EXP_GROUP)
    second_offset = jax.random.randint(k_second, (span_count, GROUPS), 0, EXP_GROUP - 1)
    first_pick = (local_rank + jnp.take_along_axis(first_offset, group_id, axis=1)) % EXP_GROUP
    second_step = (local_rank // EXP_GROUP + jnp.take_along_axis(second_offset, group_id, axis=1)) % (EXP_GROUP - 1)
    second_pick = (first_pick + 1 + second_step) % EXP_GROUP
    chosen = jnp.stack([group_id * EXP_GROUP + first_pick, group_id * EXP_GROUP + second_pick], axis=-1)
    return chosen.reshape(TOKENS_MOE, 2).astype(jnp.int32)


def block_levels(stream_key, dims, cuts, least, high):
    def one(dim, shards_of):
        draws = jax.random.uniform(jax.random.fold_in(jax.random.fold_in(stream_key, 6), dim), (shards_of,), jnp.float32, least / len(cuts), high / len(cuts))
        return jnp.repeat(jnp.exp(draws), dims[dim] // shards_of).reshape((-1,) + (1,) * (len(dims) - dim - 1))

    gain = one(*cuts[0])
    for cut in cuts[1:]:
        gain = gain * one(*cut)
    return gain


def centred(own_key, extent, scale, limit, cuts=(), kind=jnp.bfloat16):
    level = block_levels(own_key, extent, cuts, -0.22, 0.18) if cuts else 1.0
    drawn = jax.random.normal(own_key, extent, jnp.float32) * scale * level
    return jnp.minimum(jnp.maximum(drawn, -limit), limit).astype(kind)


def setup_inputs(seed: int = 0) -> dict:
    arg_keys = jax.random.split(jax.random.key(seed), 14)
    queries = centred(arg_keys[0], (MIXER_TOKENS, RETENTION_HEADS * HEAD_DIM), 1.0, 6.0, ((0, 32), (1, 16)))
    keys = centred(arg_keys[1], (MIXER_TOKENS, RETENTION_HEADS * HEAD_DIM), 1.0, 6.0, ((0, 32), (1, 16)))
    values = centred(arg_keys[2], (MIXER_TOKENS, RETENTION_HEADS * HEAD_DIM), 1.0, 6.0, ((0, 32), (1, 16)))
    gates = centred(arg_keys[3], (MIXER_TOKENS, RETENTION_HEADS * HEAD_DIM), 1.0, 6.0, ((0, 32), (1, 16)))
    log_decay = draw_log_decay(jax.random.fold_in(arg_keys[13], 71), 0)
    out_weight = centred(arg_keys[5], (RETENTION_HEADS * HEAD_DIM, D), (RETENTION_HEADS * HEAD_DIM) ** -0.5, 0.125, ((1, 16),))
    moe_rows = draw_moe_rows(jax.random.fold_in(arg_keys[13], 71), 0)
    moe_gain = jnp.clip(1.0 + 0.18 * jax.random.normal(arg_keys[7], (D,), jnp.float32), 0.099609375, 1.8984375).astype(jnp.bfloat16)
    routes = draw_routes(jax.random.fold_in(arg_keys[13], 71), 0)
    route_weights = jnp.clip(0.1 + 0.9 * jax.random.uniform(arg_keys[9], (TOKENS_MOE, 2), jnp.float32) ** block_levels(arg_keys[9], (TOKENS_MOE, 2), ((0, 32),), -0.2, 0.2), 0.1, 1.0)
    gate_proj = centred(arg_keys[10], (EXPERTS, D, FF), D ** -0.5, 0.125, ((0, 32), (2, 16)))
    up_proj = centred(arg_keys[11], (EXPERTS, D, FF), D ** -0.5, 0.125, ((0, 32), (2, 16)))
    down_proj = centred(arg_keys[12], (EXPERTS, FF, D), FF ** -0.5, 0.09375, ((0, 32), (2, 16)))
    return {"queries": queries, "keys": keys, "values": values, "gates": gates, "log_decay": log_decay, "out_weight": out_weight, "moe_rows": moe_rows, "moe_gain": moe_gain, "routes": routes, "route_weights": route_weights, "gate_proj": gate_proj, "up_proj": up_proj, "down_proj": down_proj}


def rotate(source, factor):
    length = source.shape[0]
    values_f = source.astype(jnp.float32).reshape(length, RETENTION_HEADS, HEAD_DIM)
    half_dim = HEAD_DIM // 2
    inverse = 10000.0 ** (-jnp.arange(half_dim, dtype=jnp.float32) / half_dim)
    angles = jnp.arange(length, dtype=jnp.float32)[:, None] * inverse[None, :]
    cosine = jnp.cos(angles)[:, None, :]
    sine_part = jnp.sin(angles)[:, None, :]
    first_half = values_f[..., :half_dim]
    second_half = values_f[..., half_dim:]
    turned = jnp.concatenate([first_half * cosine - second_half * sine_part, first_half * sine_part + second_half * cosine], axis=-1)
    return (turned * factor).astype(jnp.bfloat16)

def retention_ref(queries, keys, values, gates, log_decay, out_weight):
    length = queries.shape[0]
    block_count = length // BLOCK
    rot_q = rotate(queries, 1.0)
    rot_k = rotate(keys, HEAD_DIM ** (-0.5))
    q_blocks = rot_q.reshape(block_count, BLOCK, RETENTION_HEADS, HEAD_DIM)
    k_blocks = rot_k.reshape(block_count, BLOCK, RETENTION_HEADS, HEAD_DIM)
    v_blocks = values.reshape(block_count, BLOCK, RETENTION_HEADS, HEAD_DIM)
    l_blocks = log_decay.reshape(block_count, BLOCK, RETENTION_HEADS)
    causal = jnp.arange(BLOCK)[:, None] >= jnp.arange(BLOCK)[None, :]

    def advance(carry_state, member):
        q_block, k_block, v_block, l_block = member
        cumulative = jnp.cumsum(l_block, axis=0)
        across = cumulative.T
        spread = across[:, :, None] - across[:, None, :]
        weights = jnp.where(causal, jnp.exp(jnp.where(causal, spread, 0.0)), 0.0)
        q_float = q_block.astype(jnp.float32)
        k_float = k_block.astype(jnp.float32)
        v_float = v_block.astype(jnp.float32)
        scores = jnp.einsum('ihd,jhd->hij', q_float, k_float)
        rounded = lax.optimization_barrier((scores * weights).astype(jnp.bfloat16)).astype(jnp.float32)
        inside = jnp.einsum('hij,jhd->ihd', rounded, v_float)
        carried = jnp.einsum('ihd,hde->ihe', q_float, carry_state, precision=lax.Precision.HIGHEST) * jnp.exp(cumulative)[:, :, None]
        ending = cumulative[-1]
        k_scaled = k_float * jnp.exp(ending[None, :] - cumulative)[:, :, None]
        update = jnp.einsum('jhd,jhe->hde', k_scaled, v_float, precision=lax.Precision.HIGHEST)
        return (jnp.exp(ending)[:, None, None] * carry_state + update, inside + carried)
    zero_state = jnp.zeros((RETENTION_HEADS, HEAD_DIM, HEAD_DIM), jnp.float32)
    _, retained = lax.scan(advance, zero_state, (q_blocks, k_blocks, v_blocks, l_blocks))
    retained = retained.reshape(length, RETENTION_HEADS, HEAD_DIM)
    gate_f = gates.astype(jnp.float32).reshape(length, RETENTION_HEADS, HEAD_DIM)
    scaled = retained * lax.rsqrt(lax.optimization_barrier(jnp.mean(retained * retained, axis=-1, keepdims=True)) + 1e-05)
    head_out = (scaled * jax.nn.silu(gate_f)).astype(jnp.bfloat16).reshape(length, RETENTION_HEADS * HEAD_DIM)
    return jnp.dot(head_out, out_weight, preferred_element_type=jnp.float32).astype(jnp.bfloat16)

def experts_ref(moe_rows, moe_gain, routes, route_weights, gate_proj, up_proj, down_proj):
    as_float = moe_rows.astype(jnp.float32)
    normed = (as_float * lax.rsqrt(lax.optimization_barrier(jnp.mean(as_float * as_float, axis=-1, keepdims=True)) + 1e-06) * moe_gain.astype(jnp.float32)).astype(jnp.bfloat16)
    flat_ids = routes.reshape(-1)
    sorted_slots = jnp.argsort(flat_ids, stable=True).astype(jnp.int32)
    per_expert = flat_ids.shape[0] // EXPERTS
    grouped = normed[sorted_slots // 2].reshape(EXPERTS, per_expert, D)

    def run_expert(member):
        block_rows, w_gate, w_up, w_down = member
        gate_part = jnp.dot(block_rows, w_gate, preferred_element_type=jnp.float32)
        up_part = jnp.dot(block_rows, w_up, preferred_element_type=jnp.float32)
        hidden = (jax.nn.silu(gate_part) * up_part).astype(jnp.bfloat16)
        return jnp.dot(hidden, w_down, preferred_element_type=jnp.float32).astype(jnp.bfloat16)
    outputs = lax.map(run_expert, (grouped, gate_proj, up_proj, down_proj))
    slot_out = jnp.zeros((flat_ids.shape[0], D), jnp.bfloat16).at[sorted_slots].set(outputs.reshape(-1, D))
    weighted = slot_out.astype(jnp.float32).reshape(-1, 2, D) * route_weights[:, :, None]
    return lax.optimization_barrier(jnp.sum(weighted, axis=1)).astype(jnp.bfloat16)

def reference(queries, keys, values, gates, log_decay, out_weight, moe_rows, moe_gain, routes, route_weights, gate_proj, up_proj, down_proj):
    mixer_out = retention_ref(queries, keys, values, gates, log_decay, out_weight)
    moe_out = experts_ref(moe_rows, moe_gain, routes, route_weights, gate_proj, up_proj, down_proj)
    return (mixer_out, moe_out)
```

```python
import jax
import jax.numpy as jnp
import numpy as np
from jax import lax
from jax.experimental import pallas as pl
from jax.experimental.pallas import tpu as pltpu
from jax.sharding import Mesh
from jax.sharding import PartitionSpec as P

MESH = pl.DeviceIdType.MESH
F32 = jnp.float32
BF16 = jnp.bfloat16
Z, C, Y, X = 16, 2, 4, 4
E = Z * C
T = Y * X
ROWS = 256
SLOTS = 2 * ROWS
CAP = SLOTS // E
D = 2048
W = 128
BLOCK = 128
EP = ("ep_0", "ep_1")
TP = ("tp_0", "tp_1")


def mm(a, b, ca=1, cb=0):
    return lax.dot_general(a, b, (((ca,), (cb,)), ((), ())), preferred_element_type=F32)


def parts_of(a, count):
    found = []
    for k in range(count):
        piece = a.astype(BF16)
        found.append(piece)
        if k + 1 < count:
            a = a - piece.astype(F32)
    return found


def silu(v):
    return v / (1.0 + jnp.exp(-v))


class Copies:
    def __init__(self, send, recv, place):
        self.send, self.recv, self.place = send, recv, place
        self.count = 0
        self.sent = []

    def ids(self, n):
        first = self.count
        self.count += n
        return first

    def make(self, k, src, dst, dev):
        return pltpu.make_async_remote_copy(
            src_ref=src,
            dst_ref=dst,
            send_sem=self.send.at[k],
            recv_sem=self.recv.at[k],
            device_id=dev,
            device_id_type=MESH,
        )

    def start(self, k, src, dst, dev):
        copy = self.make(k, src, dst, dev)
        copy.start()
        self.sent.append(copy)

    def landed(self, k, region, dev):
        self.make(k, region, region, dev).wait_recv()

    def drain(self):
        for copy in self.sent:
            copy.wait_send()
        self.sent = []


class Spread:
    def __init__(self, copies, buf, h0, n, first):
        self.c, self.buf, self.h0, self.n, self.first = copies, buf, h0, n, first
        self.k = copies.ids(20)

    def offset(self, dp, dq):
        y, x = self.c.place
        dy, dx = (dq, dp) if self.first == "x" else (dp, dq)
        return lax.rem(y + dy + Y, Y), lax.rem(x + dx + X, X)

    def ref(self, dp, dq, part=None):
        y, x = self.offset(dp, dq)
        block = y * X + x
        if part is None:
            return self.buf.at[block, pl.ds(self.h0, self.n)]
        half = self.n // 2
        return self.buf.at[block, pl.ds(self.h0 + part * half, half)]

    def dev(self, dp, dq):
        y, x = self.offset(dp, dq)
        return {"tp_0": y, "tp_1": x}

    def go(self, k, block, to, part=None):
        ref = self.ref(*block, part)
        self.c.start(self.k + k, ref, ref, self.dev(*to))

    def got(self, k, block, part=None):
        self.c.landed(self.k + k, self.ref(*block, part), self.dev(0, 1))

    def turn(self, j):
        return {0: 0, -1: 1, 1: 2, 2: 3}[j]

    def first_own(self):
        self.go(0, (0, 0), (1, 0))
        self.go(1, (0, 0), (-1, 0))

    def across(self, j):
        base = 4 + 4 * self.turn(j)
        self.go(base, (j, 0), (0, 1))
        self.go(base + 1, (j, 0), (0, -1))

    def first_left(self):
        self.got(0, (-1, 0))
        self.go(2, (-1, 0), (1, 0), 0)

    def first_right(self):
        self.got(1, (1, 0))
        self.go(3, (1, 0), (-1, 0), 1)

    def first_far(self):
        self.got(2, (2, 0), 0)
        self.got(3, (2, 0), 1)

    def relay(self, j):
        base = 4 + 4 * self.turn(j)
        self.got(base, (j, -1))
        self.go(base + 2, (j, -1), (0, 1), 0)
        self.got(base + 1, (j, 1))
        self.go(base + 3, (j, 1), (0, -1), 1)

    def far(self, j):
        base = 4 + 4 * self.turn(j)
        self.got(base + 2, (j, 2), 0)
        self.got(base + 3, (j, 2), 1)


def both(pair, step, *args):
    for half in pair:
        getattr(half, step)(*args)


def kernel(
    q_ref, k_ref, v_ref, g_ref, ld_ref, wo_hbm, rows_ref, gain_ref, routes_ref, rw_ref,
    wg_hbm, wu_hbm, wd_hbm, cr_ref, sr_ref, cb_ref, sb_ref,
    mix_ref, moe_ref,
    wg, wu, wo, wa, wb, oh, snd, rbuf, acc, ha, hb, pa, pb, ra, rb, eo, ret,
    sts, str_, sto, sti, ins, rotq, cum, upd, ho,
    lsem, send, recv, zsem,
):
    z, c = lax.axis_index("ep_0"), lax.axis_index("ep_1")
    y, x = lax.axis_index("tp_0"), lax.axis_index("tp_1")
    e = z * C + c
    t = y * X + x
    copies = Copies(send, recv, (y, x))

    barrier = pltpu.get_barrier_semaphore()

    def ring_dev(d):
        j = lax.rem(e + d, E)
        return j, {"ep_0": j // C, "ep_1": lax.rem(j, C)}

    def greet(d, _):
        pl.semaphore_signal(barrier, inc=1, device_id=ring_dev(d)[1], device_id_type=MESH)
        return _

    lax.fori_loop(1, E, greet, 0)
    for s in range(1, 4):
        pl.semaphore_signal(
            barrier, inc=1, device_id={"tp_0": lax.rem(y + s, Y)}, device_id_type=MESH
        )
        pl.semaphore_signal(
            barrier, inc=1, device_id={"tp_1": lax.rem(x + s, X)}, device_id_type=MESH
        )

    wd_rows = wd_hbm
    local = [
        pltpu.make_async_copy(wg_hbm, wg, lsem.at[0]),
        pltpu.make_async_copy(wu_hbm, wu, lsem.at[1]),
        pltpu.make_async_copy(wd_rows.at[y, :, 0], wa.at[y], lsem.at[2]),
        pltpu.make_async_copy(wd_rows.at[:, x, 1], wb.at[x], lsem.at[3]),
        pltpu.make_async_copy(wo_hbm, wo, lsem.at[4]),
    ]
    for copy in local:
        copy.start()

    slot_id = lax.broadcasted_iota(jnp.int32, (SLOTS, ROWS), 0)
    expert_of = slot_id // CAP
    place_of = (slot_id - expert_of * CAP).astype(F32)
    named = [routes_ref[k : k + 1, :] == expert_of for k in range(2)]
    either = jnp.logical_or(named[0], named[1])
    before = (
        lax.broadcasted_iota(jnp.int32, (ROWS, ROWS), 0)
        < lax.broadcasted_iota(jnp.int32, (ROWS, ROWS), 1)
    )
    rank = mm(either.astype(F32).astype(BF16), before.astype(F32).astype(BF16))
    here = rank == place_of
    for k in range(2):
        oh[k] = jnp.logical_and(named[k], here).astype(F32).astype(BF16)

    lanes = pl.ds(pl.multiple_of(t * W, W), W)

    def squares(r, _):
        rows = pl.ds(pl.multiple_of(r * 64, 64), 64)
        full = rows_ref[rows, :].astype(F32)
        mean = jnp.sum(full * full, axis=-1, keepdims=True) * (1.0 / D)
        mine = rows_ref[rows, lanes].astype(F32)
        normed = mine * lax.rsqrt(mean + 1e-06) * gain_ref[:, lanes].astype(F32)
        rotq[rows, :] = normed.astype(BF16)
        return _

    lax.fori_loop(0, ROWS // 64, squares, 0)
    normed = rotq[...]
    picked = mm(oh[0] + oh[1], normed)
    snd[...] = picked.astype(BF16)
    mine_at = pl.ds(pl.multiple_of(e * CAP, CAP), CAP)
    rbuf[t, mine_at, :] = snd[mine_at, :]

    pl.semaphore_wait(barrier, E - 1 + 6)

    def far_first(i):
        half = (i + 1) // 2
        return E // 2 + half * (1 - 2 * lax.rem(i, 2))

    def dispatch(i, _):
        j, dev = ring_dev(far_first(i))
        pltpu.make_async_remote_copy(
            src_ref=snd.at[pl.ds(pl.multiple_of(j * CAP, CAP), CAP)],
            dst_ref=rbuf.at[t, mine_at],
            send_sem=zsem.at[0],
            recv_sem=zsem.at[1],
            device_id=dev,
            device_id_type=MESH,
        ).start()
        return _

    lax.fori_loop(0, E - 1, dispatch, 0)

    wk = copies.ids(6)
    for s in (2, 1, 3):
        yy, xx = lax.rem(y + s, Y), lax.rem(x + s, X)
        copies.start(wk + s - 1, wd_rows.at[yy, :, 0], wa.at[y], {"tp_0": yy})
        copies.start(wk + 2 + s, wd_rows.at[:, xx, 1], wb.at[x], {"tp_1": xx})

    cb, sb = cb_ref[e], sb_ref[e]
    cos = cb * cr_ref[...] - sb * sr_ref[...]

    def signed(first, second):
        lane = lax.broadcasted_iota(jnp.int32, first.shape, 1)
        return jnp.where(lane < W // 2, -first, second)

    sin = sb * cr_ref[...] + cb * sr_ref[...]
    sin = signed(sin, sin)

    def turned(ref):
        full = ref[...].astype(F32)
        return full * cos + pltpu.roll(full, W // 2, 1) * sin

    rq = turned(q_ref).astype(BF16)
    rotq[...] = rq
    rk = (turned(k_ref) * (W**-0.5)).astype(BF16)
    row_i = lax.broadcasted_iota(jnp.int32, (BLOCK, BLOCK), 0)
    col_i = lax.broadcasted_iota(jnp.int32, (BLOCK, BLOCK), 1)
    causal = row_i >= col_i
    tri = causal.astype(F32).astype(BF16)
    ends = []
    for b in range(2):
        rows = slice(b * BLOCK, (b + 1) * BLOCK)
        decay = jnp.broadcast_to(ld_ref[b : b + 1, :], (BLOCK, BLOCK))
        column = jnp.zeros((BLOCK, BLOCK), F32)
        line = jnp.zeros((BLOCK, BLOCK), F32)
        for piece in parts_of(decay, 3):
            column = column + mm(tri, piece, 1, 1)
            line = line + mm(piece, tri, 1, 1)
        spread = column - line
        factor = jnp.where(causal, jnp.exp(jnp.where(causal, spread, 0.0)), 0.0)
        weights = (mm(rq[rows], rk[rows], 1, 1) * factor).astype(BF16)
        values = v_ref[rows, :]
        cum[rows, :] = column
        end = column[BLOCK - 1 : BLOCK, :]
        ends.append(end)
        scaled = rk[rows].astype(F32) * jnp.exp(end - column)
        high, low = parts_of(scaled, 2)
        upd[b] = mm(high, values, 0, 0) + mm(low, values, 0, 0)
        acc[rows, 0:W] = mm(weights, values)
    whole = jnp.exp(ends[1]) * upd[0] + upd[1]
    total = ends[0] + ends[1]
    for s in range(Z):
        sts[s, 0:8, :] = whole[s * 8 : (s + 1) * 8, :]
        sts[s, 8:9, :] = total
    upd[1] = jnp.broadcast_to(jnp.exp(ends[0]), (BLOCK, W))
    inside = acc[0:ROWS, 0:W]
    ins[...] = inside

    owner = c == lax.rem(z, C)
    str_[e] = sts[z]

    def give(i, carry):
        s = lax.rem(z + i, Z)

        @pl.when(jnp.logical_or(i > 0, jnp.logical_not(owner)))
        def _():
            pltpu.make_async_remote_copy(
                src_ref=sts.at[s],
                dst_ref=str_.at[e],
                send_sem=zsem.at[4],
                recv_sem=zsem.at[5],
                device_id={"ep_0": s, "ep_1": lax.rem(s, C)},
                device_id_type=MESH,
            ).start()

        return carry

    lax.fori_loop(0, Z, give, 0)

    def z_all(buf, sem, kind):
        part = buf.at[pl.ds(0, (E - 1) * CAP)]
        copy = pltpu.make_async_remote_copy(
            src_ref=part, dst_ref=part, send_sem=zsem.at[sem], recv_sem=zsem.at[sem],
            device_id={"tp_1": lax.rem(x + 1, X)}, device_id_type=MESH,
        )
        if kind == "recv":
            copy.wait_recv()
        else:
            copy.wait_send()

    z_all(rbuf.at[t], 1, "recv")
    moe = (Spread(copies, rbuf, 0, ROWS, "x"), Spread(copies, rbuf, ROWS, ROWS, "y"))
    both(moe, "first_own")
    both(moe, "across", 0)

    def state_all(buf, count, sem, kind):
        part = buf.at[pl.ds(0, count)]
        copy = pltpu.make_async_remote_copy(
            src_ref=part, dst_ref=part, send_sem=zsem.at[sem], recv_sem=zsem.at[sem],
            device_id={"tp_1": lax.rem(x + 1, X)}, device_id_type=MESH,
        )
        if kind == "recv":
            copy.wait_recv()
        else:
            copy.wait_send()

    @pl.when(owner)
    def _():
        state_all(str_, E - 1, 5, "recv")
        current = jnp.zeros((8, W), F32)
        for j in range(E):
            sto[j] = current
            if j + 1 < E:
                current = jnp.exp(str_[j, 8:9, :]) * current + str_[j, 0:8, :]
        sti[z] = sto[e]

        def back(i, _):
            j, dev = ring_dev(far_first(i))
            pltpu.make_async_remote_copy(
                src_ref=sto.at[j],
                dst_ref=sti.at[z],
                send_sem=zsem.at[6],
                recv_sem=zsem.at[7],
                device_id=dev,
                device_id_type=MESH,
            ).start()
            return _

        lax.fori_loop(0, E - 1, back, 0)

    both(moe, "first_left")
    both(moe, "across", -1)
    both(moe, "first_right")
    both(moe, "across", 1)
    both(moe, "relay", 0)
    both(moe, "first_far")
    both(moe, "across", 2)

    local[0].wait()
    local[1].wait()

    def gather_group(half, dq, fresh):
        rows = pl.ds(half.h0, half.n)
        blocks, left = [], []
        for k in range(4):
            yy, xx = half.offset(k, dq)
            blocks.append(yy * X + xx)
        left = jnp.concatenate([rbuf[b, rows, :] for b in blocks], axis=1)
        for at, weight in ((0, wg), (256, wu)):
            right = jnp.concatenate(
                [weight[pl.ds(pl.multiple_of(b * W, W), W), :] for b in blocks], axis=0
            )
            product = mm(left, right)
            if fresh:
                acc[rows, at : at + 256] = product
            else:
                acc[rows, at : at + 256] += product

    for half in moe:
        gather_group(half, 0, True)

    @pl.when(owner)
    def _():
        state_all(sti, Z - 1, 7, "recv")

    @pl.when(jnp.logical_not(owner))
    def _():
        state_all(sti, Z, 7, "recv")

    entering = sti[...].reshape(W, W)
    for b in range(2):
        rows = slice(b * BLOCK, (b + 1) * BLOCK)
        high, low = parts_of(entering, 2)
        query = rotq[rows, :]
        carried = (mm(query, high) + mm(query, low)) * jnp.exp(cum[rows, :])
        retained = ins[rows, :] + carried
        mean = jnp.sum(retained * retained, axis=-1, keepdims=True) * (1.0 / W)
        gate = g_ref[rows, :].astype(F32)
        ho[t, rows, :] = (retained * lax.rsqrt(mean + 1e-05) * silu(gate)).astype(BF16)
        entering = upd[1] * entering + upd[0]
    mix = (Spread(copies, ho, 0, BLOCK, "x"), Spread(copies, ho, BLOCK, BLOCK, "y"))
    both(mix, "first_own")
    both(mix, "across", 0)

    both(moe, "relay", -1)
    both(moe, "relay", 1)
    both(moe, "relay", 2)
    for half in moe:
        gather_group(half, -1, False)
        gather_group(half, 1, False)
    for j in (0, -1, 1, 2):
        both(moe, "far", j)
    for half in moe:
        gather_group(half, 2, False)

    hidden = (silu(acc[:, 0:256]) * acc[:, 256:512]).astype(BF16)
    ha[x] = hidden[:, 0:W]
    hb[y] = hidden[:, W : 2 * W]

    hk = copies.ids(8)

    def hop(k, axis, buf, block, to, part=None):
        me, size = (x, X) if axis == "tp_1" else (y, Y)
        ref = buf.at[lax.rem(me + block + size, size)]
        if part is not None:
            ref = ref.at[pl.ds(part * ROWS, ROWS)]
        return k, ref, {axis: lax.rem(me + to + size, size)}

    hsides = (("tp_1", ha, hk), ("tp_0", hb, hk + 4))
    for axis, buf, k in hsides:
        for n, to in ((0, 1), (1, -1)):
            kk, ref, dev = hop(k + n, axis, buf, 0, to)
            copies.start(kk, ref, ref, dev)

    both(mix, "first_left")
    both(mix, "across", -1)
    both(mix, "first_right")
    both(mix, "across", 1)

    for n, frm, part in ((0, -1, 0), (1, 1, 1)):
        for axis, buf, k in hsides:
            kk, ref, dev = hop(k + n, axis, buf, frm, 1)
            copies.landed(kk, ref, dev)
            kk, ref, dev = hop(k + 2 + n, axis, buf, frm, -frm, part)
            copies.start(kk, ref, ref, dev)

    both(mix, "relay", 0)
    both(mix, "first_far")
    both(mix, "across", 2)

    for axis, buf, k in hsides:
        for n in range(2):
            kk, ref, dev = hop(k + 2 + n, axis, buf, 2, 1, n)
            copies.landed(kk, ref, dev)

    local[2].wait()
    local[3].wait()
    for s in range(1, 4):
        copies.landed(wk + s - 1, wa.at[lax.rem(y + Y - s, Y)], {"tp_0": lax.rem(y + s, Y)})
        copies.landed(wk + 2 + s, wb.at[lax.rem(x + X - s, X)], {"tp_1": lax.rem(x + s, X)})

    left_a = jnp.concatenate([ha[k] for k in range(X)], axis=1)
    left_b = jnp.concatenate([hb[k] for k in range(Y)], axis=1)
    pk = copies.ids(6)
    for s in (2, 1, 3):
        yy, xx = lax.rem(y + s, Y), lax.rem(x + s, X)
        pa[s - 1] = mm(left_a, wa[yy].reshape(X * W, W)).astype(BF16)
        copies.start(pk + s - 1, pa.at[s - 1], ra.at[s - 1], {"tp_0": yy})
        pb[s - 1] = mm(left_b, wb[xx].reshape(Y * W, W)).astype(BF16)
        copies.start(pk + 2 + s, pb.at[s - 1], rb.at[s - 1], {"tp_1": xx})
    acc[:, 0:W] = mm(left_a, wa[y].reshape(X * W, W)) + mm(left_b, wb[x].reshape(Y * W, W))

    both(mix, "relay", -1)
    both(mix, "relay", 1)
    both(mix, "relay", 2)

    for s in range(1, 4):
        copies.landed(pk + s - 1, ra.at[s - 1], {"tp_0": lax.rem(y + s, Y)})
        copies.landed(pk + 2 + s, rb.at[s - 1], {"tp_1": lax.rem(x + s, X)})
    summed = acc[:, 0:W]
    for s in range(3):
        summed = summed + ra[s].astype(F32) + rb[s].astype(F32)
    eo[...] = summed.astype(BF16)
    ret[mine_at, :] = eo[mine_at, :]

    def give_back(i, _):
        j, dev = ring_dev(far_first(i))
        pltpu.make_async_remote_copy(
            src_ref=eo.at[pl.ds(pl.multiple_of(j * CAP, CAP), CAP)],
            dst_ref=ret.at[mine_at],
            send_sem=zsem.at[2],
            recv_sem=zsem.at[3],
            device_id=dev,
            device_id_type=MESH,
        ).start()
        return _

    lax.fori_loop(0, E - 1, give_back, 0)

    for j in (0, -1, 1, 2):
        both(mix, "far", j)
    local[4].wait()
    heads = jnp.concatenate([ho[k] for k in range(T)], axis=1)
    mix_ref[...] = mm(heads, wo[...]).astype(BF16)

    z_all(ret, 3, "recv")
    moe_out = jnp.zeros((ROWS, W), F32)
    for k in range(2):
        moe_out = moe_out + mm(oh[k], ret[...], 0, 0) * rw_ref[:, k : k + 1]
    moe_ref[...] = moe_out.astype(BF16)

    copies.drain()
    z_all(snd, 0, "send")
    z_all(eo, 2, "send")

    @pl.when(owner)
    def _():
        state_all(sts, Z - 1, 4, "send")
        state_all(sto, E - 1, 6, "send")

    @pl.when(jnp.logical_not(owner))
    def _():
        state_all(sts, Z, 4, "send")


def tables():
    half = W // 2
    inverse = 10000.0 ** (-np.arange(half, dtype=np.float64) / half)
    near = np.arange(ROWS, dtype=np.float64)[:, None] * inverse[None, :]
    base = (np.arange(E, dtype=np.float64) * ROWS)[:, None] * inverse[None, :]
    both_halves = lambda a: np.concatenate([a, a], axis=1).astype(np.float32)
    return (
        both_halves(np.cos(near)),
        both_halves(np.sin(near)),
        both_halves(np.cos(base))[:, None, :],
        both_halves(np.sin(base))[:, None, :],
    )


def on_device(
    queries, keys, values, gates, log_decay, out_weight,
    moe_rows, moe_gain, routes, route_weights, gate_proj, up_proj, down_proj,
):
    vmem = pl.BlockSpec(memory_space=pltpu.VMEM)
    hbm = pl.BlockSpec(memory_space=pl.ANY)
    scratch = [
        pltpu.VMEM((D, 256), BF16),
        pltpu.VMEM((D, 256), BF16),
        pltpu.VMEM((D, W), BF16),
        pltpu.VMEM((Y, X, W, W), BF16),
        pltpu.VMEM((X, Y, W, W), BF16),
        pltpu.VMEM((2, SLOTS, ROWS), BF16),
        pltpu.VMEM((SLOTS, W), BF16),
        pltpu.VMEM((T, SLOTS, W), BF16),
        pltpu.VMEM((SLOTS, 512), F32),
        pltpu.VMEM((X, SLOTS, W), BF16),
        pltpu.VMEM((Y, SLOTS, W), BF16),
        pltpu.VMEM((3, SLOTS, W), BF16),
        pltpu.VMEM((3, SLOTS, W), BF16),
        pltpu.VMEM((3, SLOTS, W), BF16),
        pltpu.VMEM((3, SLOTS, W), BF16),
        pltpu.VMEM((SLOTS, W), BF16),
        pltpu.VMEM((SLOTS, W), BF16),
        pltpu.VMEM((Z, 9, W), F32),
        pltpu.VMEM((E, 9, W), F32),
        pltpu.VMEM((E, 8, W), F32),
        pltpu.VMEM((Z, 8, W), F32),
        pltpu.VMEM((ROWS, W), F32),
        pltpu.VMEM((ROWS, W), BF16),
        pltpu.VMEM((ROWS, W), F32),
        pltpu.VMEM((2, W, W), F32),
        pltpu.VMEM((T, ROWS, W), BF16),
        pltpu.SemaphoreType.DMA((5,)),
        pltpu.SemaphoreType.DMA((100,)),
        pltpu.SemaphoreType.DMA((100,)),
        pltpu.SemaphoreType.DMA((8,)),
    ]
    out = jax.ShapeDtypeStruct((ROWS, W), BF16)
    return pl.pallas_call(
        kernel,
        out_shape=(out, out),
        in_specs=[vmem] * 5 + [hbm] + [vmem] * 4 + [hbm] * 3 + [vmem] * 4,
        out_specs=(vmem, vmem),
        scratch_shapes=scratch,
        compiler_params=pltpu.CompilerParams(
            collective_id=0, has_side_effects=True, vmem_limit_bytes=48 * 2**20
        ),
    )(
        queries, keys, values, gates, log_decay.reshape(2, BLOCK), out_weight,
        moe_rows, moe_gain.reshape(1, D), routes.T, route_weights,
        gate_proj.reshape(D, 256), up_proj.reshape(D, 256),
        down_proj.reshape(Y, X, 2, W, W), *tables(),
    )


def solution(mesh):
    torus = Mesh(mesh.devices.reshape(Z, C, Y, X), ("ep_0", "ep_1", "tp_0", "tp_1"))
    return jax.shard_map(
        on_device,
        mesh=torus,
        in_specs=(
            P(EP, TP), P(EP, TP), P(EP, TP), P(EP, TP), P(EP, TP), P(None, TP),
            P(EP, None), P(), P(EP, None), P(EP, None),
            P(EP, None, TP), P(EP, None, TP), P(EP, None, TP),
        ),
        out_specs=(P(EP, TP), P(EP, TP)),
        check_vma=False,
    )
```

```python
import jax
import jax.numpy as jnp
import numpy as np
from jax import lax
from jax.experimental import pallas as pl
from jax.experimental.pallas import tpu as pltpu
from jax.sharding import Mesh
from jax.sharding import PartitionSpec as P

MESH = pl.DeviceIdType.MESH
F32 = jnp.float32
BF16 = jnp.bfloat16
Z, C, Y, X = 16, 2, 4, 4
E = Z * C
T = Y * X
ROWS = 256
SLOTS = 2 * ROWS
CAP = SLOTS // E
D = 2048
W = 128
BLOCK = 128
NEAR = 8
EP = ("ep_0", "ep_1")
TP = ("tp_0", "tp_1")


def mm(a, b, ca=1, cb=0):
    return lax.dot_general(a, b, (((ca,), (cb,)), ((), ())), preferred_element_type=F32)


def parts_of(a, count):
    found = []
    for k in range(count):
        piece = a.astype(BF16)
        found.append(piece)
        if k + 1 < count:
            a = a - piece.astype(F32)
    return found


def silu(v):
    return v / (1.0 + jnp.exp(-v))


class Copies:
    def __init__(self, send, recv, place):
        self.send, self.recv, self.place = send, recv, place
        self.count = 0
        self.sent = []

    def ids(self, n):
        first = self.count
        self.count += n
        return first

    def make(self, k, src, dst, dev):
        return pltpu.make_async_remote_copy(
            src_ref=src,
            dst_ref=dst,
            send_sem=self.send.at[k],
            recv_sem=self.recv.at[k],
            device_id=dev,
            device_id_type=MESH,
        )

    def start(self, k, src, dst, dev):
        copy = self.make(k, src, dst, dev)
        copy.start()
        self.sent.append(copy)

    def landed(self, k, region, dev):
        self.make(k, region, region, dev).wait_recv()

    def drain(self):
        for copy in self.sent:
            copy.wait_send()
        self.sent = []


class Spread:
    def __init__(self, copies, buf, h0, n, axis):
        self.c, self.buf, self.h0, self.n, self.axis = copies, buf, h0, n, axis
        self.k = copies.ids(20)

    def offset(self, dp, dq):
        y, x = self.c.place
        dy, dx = (dq, dp) if self.axis == "x" else (dp, dq)
        return lax.rem(y + dy + Y, Y), lax.rem(x + dx + X, X)

    def ref(self, dp, dq, part=None):
        y, x = self.offset(dp, dq)
        block = y * X + x
        if part is None:
            return self.buf.at[block, pl.ds(self.h0, self.n)]
        half = self.n // 2
        return self.buf.at[block, pl.ds(self.h0 + part * half, half)]

    def dev(self, dp, dq):
        y, x = self.offset(dp, dq)
        return {"tp_0": y, "tp_1": x}

    def go(self, k, block, to, part=None):
        ref = self.ref(*block, part)
        self.c.start(self.k + k, ref, ref, self.dev(*to))

    def got(self, k, block, part=None):
        self.c.landed(self.k + k, self.ref(*block, part), self.dev(0, 1))

    def turn(self, j):
        return {0: 0, -1: 1, 1: 2, 2: 3}[j]

    def own(self):
        for k, to in enumerate(((1, 0), (-1, 0), (2, 0))):
            self.go(k, (0, 0), to)
        self.go(4, (0, 0), (0, 1))
        self.go(5, (0, 0), (0, -1))

    def across(self, j):
        base = 4 + 4 * self.turn(j)
        for k, to in enumerate((1, -1, 2)):
            self.go(base + k, (j, 0), (0, to))

    def first(self):
        for k, j in enumerate((-1, 1, 2)):
            self.got(k, (j, 0))
            self.across(j)

    def relay(self):
        self.got(4, (0, -1))
        self.go(6, (0, -1), (0, 1), 0)
        self.got(5, (0, 1))
        self.go(7, (0, 1), (0, -1), 1)

    def near(self):
        for j in (-1, 1, 2):
            base = 4 + 4 * self.turn(j)
            self.got(base, (j, -1))
            self.got(base + 1, (j, 1))

    def far(self):
        self.got(6, (0, 2), 0)
        self.got(7, (0, 2), 1)
        for j in (-1, 1, 2):
            self.got(4 + 4 * self.turn(j) + 2, (j, 2))


def both(pair, step, *args):
    for half in pair:
        getattr(half, step)(*args)


def kernel(
    q_hbm, k_hbm, v_hbm, g_hbm, ld_hbm, wo_hbm, rows_hbm, gain_hbm, routes_hbm, rw_hbm,
    wg_hbm, wu_hbm, wd_hbm, cr_hbm, sr_hbm, cb_hbm, sb_hbm,
    mix_hbm, moe_hbm,
    q_ref, k_ref, v_ref, g_ref, ld_ref, rows_ref, gain_ref, routes_ref, rw_ref,
    cr_ref, sr_ref, cb_ref, sb_ref, mix_ref, moe_ref,
    wg, wu, wo, wa, wb, oh, snd, rbuf, acc, ha, hb, pa, pb, ra, rb, eo, ret,
    sts, str_, sto, sti, ins, rotq, cum, upd, ho, psum,
    lsem, send, recv, zsem,
):
    z, c = lax.axis_index("ep_0"), lax.axis_index("ep_1")
    y, x = lax.axis_index("tp_0"), lax.axis_index("tp_1")
    e = z * C + c
    t = y * X + x
    copies = Copies(send, recv, (y, x))

    barrier = pltpu.get_barrier_semaphore()
    wd_rows = wd_hbm
    routed = (
        (routes_hbm, routes_ref), (rows_hbm, rows_ref), (gain_hbm, gain_ref), (rw_hbm, rw_ref),
    )
    mixed = (
        (k_hbm, k_ref), (q_hbm, q_ref), (v_hbm, v_ref), (ld_hbm, ld_ref), (cr_hbm, cr_ref),
        (sr_hbm, sr_ref), (cb_hbm.at[e], cb_ref), (sb_hbm.at[e], sb_ref), (g_hbm, g_ref),
    )
    held = (
        (wg_hbm, wg), (wu_hbm, wu), (wd_rows.at[y, :, 0], wa.at[y]),
        (wd_rows.at[:, x, 1], wb.at[x]), (wo_hbm, wo),
    )
    local = [
        pltpu.make_async_copy(src, dst, lsem.at[n])
        for n, (src, dst) in enumerate(routed + mixed + held)
    ]
    for copy in local:
        copy.start()
    routed = local[: len(routed)]
    mixed = local[len(routed) : -len(held)]
    local = local[-len(held) :]

    def ring_dev(d):
        j = lax.rem(e + d, E)
        return j, {"ep_0": j // C, "ep_1": lax.rem(j, C)}

    def greet(d, _):
        pl.semaphore_signal(barrier, inc=1, device_id=ring_dev(d)[1], device_id_type=MESH)
        return _

    lax.fori_loop(1, E, greet, 0)
    for s in range(1, 4):
        pl.semaphore_signal(
            barrier, inc=1, device_id={"tp_0": lax.rem(y + s, Y)}, device_id_type=MESH
        )
        pl.semaphore_signal(
            barrier, inc=1, device_id={"tp_1": lax.rem(x + s, X)}, device_id_type=MESH
        )

    for copy in routed:
        copy.wait()

    slot_id = lax.broadcasted_iota(jnp.int32, (SLOTS, ROWS), 0)
    expert_of = slot_id // CAP
    place_of = (slot_id - expert_of * CAP).astype(F32)
    named = [routes_ref[k : k + 1, :] == expert_of for k in range(2)]
    either = jnp.logical_or(named[0], named[1])
    before = (
        lax.broadcasted_iota(jnp.int32, (ROWS, ROWS), 0)
        < lax.broadcasted_iota(jnp.int32, (ROWS, ROWS), 1)
    )
    rank = mm(either.astype(F32).astype(BF16), before.astype(F32).astype(BF16))
    here = rank == place_of
    for k in range(2):
        oh[k] = jnp.logical_and(named[k], here).astype(F32).astype(BF16)

    lanes = pl.ds(pl.multiple_of(t * W, W), W)
    gain_at = lax.broadcasted_iota(jnp.int32, (T, W), 0) == t
    gain = jnp.sum(jnp.where(gain_at, gain_ref[...].astype(F32), 0.0), axis=0, keepdims=True)

    def squares(r, _):
        rows = pl.ds(pl.multiple_of(r * 64, 64), 64)
        full = rows_ref[rows, :].astype(F32)
        mean = jnp.sum(full * full, axis=-1, keepdims=True) * (1.0 / D)
        mine = rows_ref[rows, lanes].astype(F32)
        normed = mine * lax.rsqrt(mean + 1e-06) * gain
        rotq[rows, :] = normed.astype(BF16)
        return _

    lax.fori_loop(0, ROWS // 64, squares, 0)
    normed = rotq[...]
    picked = mm(oh[0] + oh[1], normed)
    snd[...] = picked.astype(BF16)
    mine_at = pl.ds(pl.multiple_of(e * CAP, CAP), CAP)
    own_rows = slice(NEAR * CAP, (NEAR + 1) * CAP)
    rbuf[t, own_rows, :] = snd[mine_at, :]

    pl.semaphore_wait(barrier, E - 1 + 6)

    def near_d(i):
        even = 1 - lax.rem(i, 2)
        return even * (i // 2 - NEAR) + (1 - even) * (NEAR - 1 - i // 2)

    def far_d(i):
        half = (i + 1) // 2
        return E // 2 + half * (1 - 2 * lax.rem(i, 2))

    def tile(k):
        return pl.ds(pl.multiple_of(k * CAP, CAP), CAP)

    def dispatch(d, sem):
        j, dev = ring_dev(E - d)
        pltpu.make_async_remote_copy(
            src_ref=snd.at[tile(j)],
            dst_ref=rbuf.at[t, tile(NEAR + d)],
            send_sem=zsem.at[0],
            recv_sem=zsem.at[sem],
            device_id=dev,
            device_id_type=MESH,
        ).start()

    def dispatch_near(i, carry):
        dispatch(near_d(i), 1)
        return carry

    def dispatch_far(i, carry):
        dispatch(far_d(i), 8)
        return carry

    lax.fori_loop(0, E // 2 - 1, dispatch_near, 0)
    lax.fori_loop(0, E // 2, dispatch_far, 0)

    wk = copies.ids(6)
    for s in (2, 1, 3):
        yy, xx = lax.rem(y + s, Y), lax.rem(x + s, X)
        copies.start(wk + s - 1, wd_rows.at[yy, :, 0], wa.at[y], {"tp_0": yy})
        copies.start(wk + 2 + s, wd_rows.at[:, xx, 1], wb.at[x], {"tp_1": xx})

    for copy in mixed:
        copy.wait()
    cb, sb = cb_ref[...], sb_ref[...]
    cos = cb * cr_ref[...] - sb * sr_ref[...]

    def signed(first, second):
        lane = lax.broadcasted_iota(jnp.int32, first.shape, 1)
        return jnp.where(lane < W // 2, -first, second)

    sin = sb * cr_ref[...] + cb * sr_ref[...]
    sin = signed(sin, sin)

    def turned(ref):
        full = ref[...].astype(F32)
        return full * cos + pltpu.roll(full, W // 2, 1) * sin

    rq = turned(q_ref).astype(BF16)
    rotq[...] = rq
    rk = (turned(k_ref) * (W**-0.5)).astype(BF16)
    row_i = lax.broadcasted_iota(jnp.int32, (BLOCK, BLOCK), 0)
    col_i = lax.broadcasted_iota(jnp.int32, (BLOCK, BLOCK), 1)
    causal = row_i >= col_i
    tri = causal.astype(F32).astype(BF16)
    ends = []
    for b in range(2):
        rows = slice(b * BLOCK, (b + 1) * BLOCK)
        decay = jnp.broadcast_to(ld_ref[b : b + 1, :], (BLOCK, BLOCK))
        column = jnp.zeros((BLOCK, BLOCK), F32)
        line = jnp.zeros((BLOCK, BLOCK), F32)
        for piece in parts_of(decay, 3):
            column = column + mm(tri, piece, 1, 1)
            line = line + mm(piece, tri, 1, 1)
        spread = column - line
        factor = jnp.where(causal, jnp.exp(jnp.where(causal, spread, 0.0)), 0.0)
        weights = (mm(rq[rows], rk[rows], 1, 1) * factor).astype(BF16)
        values = v_ref[rows, :]
        cum[rows, :] = column
        end = column[BLOCK - 1 : BLOCK, :]
        ends.append(end)
        scaled = rk[rows].astype(F32) * jnp.exp(end - column)
        high, low = parts_of(scaled, 2)
        upd[b] = mm(high, values, 0, 0) + mm(low, values, 0, 0)
        acc[rows, 0:W] = mm(weights, values)
    whole = jnp.exp(ends[1]) * upd[0] + upd[1]
    total = ends[0] + ends[1]
    for s in range(Z):
        sts[s, 0:8, :] = whole[s * 8 : (s + 1) * 8, :]
        sts[s, 8:9, :] = total
    upd[1] = jnp.broadcast_to(jnp.exp(ends[0]), (BLOCK, W))
    inside = acc[0:ROWS, 0:W]
    ins[...] = inside

    owner = c == lax.rem(z, C)
    str_[e] = sts[z]

    def give(i, carry):
        s = lax.rem(z + i, Z)

        @pl.when(jnp.logical_or(i > 0, jnp.logical_not(owner)))
        def _():
            pltpu.make_async_remote_copy(
                src_ref=sts.at[s],
                dst_ref=str_.at[e],
                send_sem=zsem.at[4],
                recv_sem=zsem.at[5],
                device_id={"ep_0": s, "ep_1": lax.rem(s, C)},
                device_id_type=MESH,
            ).start()

        return carry

    lax.fori_loop(0, Z, give, 0)

    def tiles(buf, count, sem, kind):
        part = buf.at[pl.ds(0, count * CAP)]
        copy = pltpu.make_async_remote_copy(
            src_ref=part, dst_ref=part, send_sem=zsem.at[sem], recv_sem=zsem.at[sem],
            device_id={"tp_1": lax.rem(x + 1, X)}, device_id_type=MESH,
        )
        if kind == "recv":
            copy.wait_recv()
        else:
            copy.wait_send()

    HALF = ROWS // 2
    moe = [
        (
            Spread(copies, rbuf, ROWS * n, HALF, "x"),
            Spread(copies, rbuf, ROWS * n + HALF, HALF, "y"),
        )
        for n in range(2)
    ]
    hop_ids = [copies.ids(8) for _ in range(2)]
    sum_ids = [copies.ids(6) for _ in range(2)]

    def chunk(n):
        return slice(n * ROWS, (n + 1) * ROWS)

    def spread_own(n):
        tiles(rbuf.at[t], E // 2 - 1 + n, 1 if n == 0 else 8, "recv")
        both(moe[n], "own")

    def spread_first(n):
        both(moe[n], "first")
        both(moe[n], "relay")

    def gather_group(half, dqs, fresh):
        rows = pl.ds(half.h0, half.n)
        blocks = []
        for dq in dqs:
            for k in range(4):
                yy, xx = half.offset(k, dq)
                blocks.append(yy * X + xx)
        left = jnp.concatenate([rbuf[b, rows, :] for b in blocks], axis=1)
        for at, weight in ((0, wg), (256, wu)):
            right = jnp.concatenate(
                [weight[pl.ds(pl.multiple_of(b * W, W), W), :] for b in blocks], axis=0
            )
            product = mm(left, right)
            if fresh:
                acc[rows, at : at + 256] = product
            else:
                acc[rows, at : at + 256] += product

    def gather(n, *dqs):
        for half in moe[n]:
            gather_group(half, dqs, dqs == (0,))

    def hop(n, side, block, to):
        axis, buf, me = (("tp_1", ha, x), ("tp_0", hb, y))[side]
        ref = buf.at[lax.rem(me + block, 4), pl.ds(n * ROWS, ROWS)]
        return hop_ids[n] + 4 * side + to, ref, {axis: lax.rem(me + to, 4)}

    def hidden_own(n):
        both(moe[n], "near")
        gather(n, 1, -1)
        both(moe[n], "far")
        gather(n, 2)
        rows = chunk(n)
        hidden = (silu(acc[rows, 0:256]) * acc[rows, 256:512]).astype(BF16)
        ha[x, rows, :] = hidden[:, 0:W]
        hb[y, rows, :] = hidden[:, W : 2 * W]
        for to in (2, 1, 3):
            for side in range(2):
                kk, ref, dev = hop(n, side, 0, to)
                copies.start(kk, ref, ref, dev)

    def partial(n, side, offsets):
        buf, weight, me, other = ((ha, wa, x, y), (hb, wb, y, x))[side]
        rows = chunk(n)
        held = [lax.rem(me + o, 4) for o in offsets]
        left = jnp.concatenate([buf[b, rows, :] for b in held], axis=1)
        right = jnp.concatenate(
            [
                jnp.concatenate([weight[lax.rem(other + s, 4), b] for b in held], axis=0)
                for s in range(4)
            ],
            axis=1,
        )
        return mm(left, right)

    def down_own(n):
        for side in range(2):
            psum[side, chunk(n), :] = partial(n, side, (0,))

    def down_rest(n):
        for side in range(2):
            for to in range(1, 4):
                kk, ref, dev = hop(n, side, 4 - to, to)
                copies.landed(kk, ref, dev)
        rows = chunk(n)
        at = pl.ds(n * ROWS, ROWS)
        for side in range(2):
            out, into, axis, me = ((pa, ra, "tp_0", y), (pb, rb, "tp_1", x))[side]
            whole = psum[side, rows, :] + partial(n, side, (1, 3, 2))
            for s in (2, 1, 3):
                out[s - 1, rows, :] = whole[:, s * W : (s + 1) * W].astype(BF16)
                copies.start(
                    sum_ids[n] + 3 * side + s - 1, out.at[s - 1, at], into.at[s - 1, at],
                    {axis: lax.rem(me + s, 4)},
                )
            psum[side, rows, 0:W] = whole[:, 0:W]

    def give_back(d):
        j, dev = ring_dev(E + d)
        pltpu.make_async_remote_copy(
            src_ref=eo.at[tile(NEAR + d)],
            dst_ref=ret.at[mine_at],
            send_sem=zsem.at[2],
            recv_sem=zsem.at[3],
            device_id=dev,
            device_id_type=MESH,
        ).start()

    def back_near(i, carry):
        give_back(near_d(i))
        return carry

    def back_far(i, carry):
        give_back(far_d(i))
        return carry

    def finish(n):
        rows = chunk(n)
        at = pl.ds(n * ROWS, ROWS)
        summed = psum[0, rows, 0:W] + psum[1, rows, 0:W]
        for side in range(2):
            into, axis, me = ((ra, "tp_0", y), (rb, "tp_1", x))[side]
            for s in range(1, 4):
                copies.landed(
                    sum_ids[n] + 3 * side + s - 1, into.at[s - 1, at], {axis: lax.rem(me + s, 4)}
                )
                summed = summed + into[s - 1, rows, :].astype(F32)
        eo[rows, :] = summed.astype(BF16)
        if n == 0:
            ret[mine_at, :] = eo[own_rows, :]
            lax.fori_loop(0, E // 2 - 1, back_near, 0)
        else:
            lax.fori_loop(0, E // 2, back_far, 0)

    spread_own(0)

    spread_first(0)
    spread_own(1)
    def state_all(buf, count, sem, kind):
        part = buf.at[pl.ds(0, count)]
        copy = pltpu.make_async_remote_copy(
            src_ref=part, dst_ref=part, send_sem=zsem.at[sem], recv_sem=zsem.at[sem],
            device_id={"tp_1": lax.rem(x + 1, X)}, device_id_type=MESH,
        )
        if kind == "recv":
            copy.wait_recv()
        else:
            copy.wait_send()

    @pl.when(owner)
    def _():
        state_all(str_, E - 1, 5, "recv")
        current = jnp.zeros((8, W), F32)
        for j in range(E):
            sto[j] = current
            if j + 1 < E:
                current = jnp.exp(str_[j, 8:9, :]) * current + str_[j, 0:8, :]
        sti[z] = sto[e]

        def back(i, _):
            j, dev = ring_dev(far_d(i))
            pltpu.make_async_remote_copy(
                src_ref=sto.at[j],
                dst_ref=sti.at[z],
                send_sem=zsem.at[6],
                recv_sem=zsem.at[7],
                device_id=dev,
                device_id_type=MESH,
            ).start()
            return _

        lax.fori_loop(0, E - 1, back, 0)

    local[0].wait()
    local[1].wait()
    gather(0, 0)
    spread_first(1)
    hidden_own(0)
    local[2].wait()
    local[3].wait()
    for s in range(1, 4):
        copies.landed(wk + s - 1, wa.at[lax.rem(y + Y - s, Y)], {"tp_0": lax.rem(y + s, Y)})
        copies.landed(wk + 2 + s, wb.at[lax.rem(x + X - s, X)], {"tp_1": lax.rem(x + s, X)})
    down_own(0)
    gather(1, 0)
    down_rest(0)
    hidden_own(1)

    @pl.when(owner)
    def _():
        state_all(sti, Z - 1, 7, "recv")

    @pl.when(jnp.logical_not(owner))
    def _():
        state_all(sti, Z, 7, "recv")

    entering = sti[...].reshape(W, W)
    for b in range(2):
        rows = slice(b * BLOCK, (b + 1) * BLOCK)
        high, low = parts_of(entering, 2)
        query = rotq[rows, :]
        carried = (mm(query, high) + mm(query, low)) * jnp.exp(cum[rows, :])
        retained = ins[rows, :] + carried
        mean = jnp.sum(retained * retained, axis=-1, keepdims=True) * (1.0 / W)
        gate = g_ref[rows, :].astype(F32)
        ho[t, rows, :] = (retained * lax.rsqrt(mean + 1e-05) * silu(gate)).astype(BF16)
        entering = upd[1] * entering + upd[0]
    mix = (Spread(copies, ho, 0, BLOCK, "x"), Spread(copies, ho, BLOCK, BLOCK, "y"))

    down_own(1)
    finish(0)
    down_rest(1)
    both(mix, "own")
    finish(1)
    both(mix, "first")
    both(mix, "relay")
    both(mix, "near")
    both(mix, "far")
    local[4].wait()
    heads = jnp.concatenate([ho[k] for k in range(T)], axis=1)
    mix_ref[...] = mm(heads, wo[...]).astype(BF16)
    mix_out = pltpu.make_async_copy(mix_ref, mix_hbm, lsem.at[0])
    mix_out.start()

    tiles(ret, E - 1, 3, "recv")
    moe_out = jnp.zeros((ROWS, W), F32)
    for k in range(2):
        share = jnp.transpose(jnp.broadcast_to(rw_ref[k : k + 1, :], (W, ROWS)))
        moe_out = moe_out + mm(oh[k], ret[...], 0, 0) * share
    moe_ref[...] = moe_out.astype(BF16)
    moe_copy = pltpu.make_async_copy(moe_ref, moe_hbm, lsem.at[1])
    moe_copy.start()

    copies.drain()
    tiles(snd, E - 1, 0, "send")
    tiles(eo, E - 1, 2, "send")

    @pl.when(owner)
    def _():
        state_all(sts, Z - 1, 4, "send")
        state_all(sto, E - 1, 6, "send")

    @pl.when(jnp.logical_not(owner))
    def _():
        state_all(sts, Z, 4, "send")
    mix_out.wait()
    moe_copy.wait()


def tables():
    half = W // 2
    inverse = 10000.0 ** (-np.arange(half, dtype=np.float64) / half)
    near = np.arange(ROWS, dtype=np.float64)[:, None] * inverse[None, :]
    base = (np.arange(E, dtype=np.float64) * ROWS)[:, None] * inverse[None, :]
    both_halves = lambda a: np.concatenate([a, a], axis=1).astype(np.float32)
    return (
        both_halves(np.cos(near)),
        both_halves(np.sin(near)),
        both_halves(np.cos(base))[:, None, :],
        both_halves(np.sin(base))[:, None, :],
    )


def on_device(
    queries, keys, values, gates, log_decay, out_weight,
    moe_rows, moe_gain, routes, route_weights, gate_proj, up_proj, down_proj,
):
    hbm = pl.BlockSpec(memory_space=pltpu.HBM)
    vmem = pl.BlockSpec(memory_space=pltpu.VMEM)
    scratch = [
        pltpu.VMEM((ROWS, W), BF16),
        pltpu.VMEM((ROWS, W), BF16),
        pltpu.VMEM((ROWS, W), BF16),
        pltpu.VMEM((ROWS, W), BF16),
        pltpu.VMEM((2, BLOCK), F32),
        pltpu.VMEM((ROWS, D), BF16),
        pltpu.VMEM((T, W), BF16),
        pltpu.VMEM((2, ROWS), jnp.int32),
        pltpu.VMEM((2, ROWS), F32),
        pltpu.VMEM((ROWS, W), F32),
        pltpu.VMEM((ROWS, W), F32),
        pltpu.VMEM((1, W), F32),
        pltpu.VMEM((1, W), F32),
        pltpu.VMEM((ROWS, W), BF16),
        pltpu.VMEM((ROWS, W), BF16),
        pltpu.VMEM((D, 256), BF16),
        pltpu.VMEM((D, 256), BF16),
        pltpu.VMEM((D, W), BF16),
        pltpu.VMEM((Y, X, W, W), BF16),
        pltpu.VMEM((X, Y, W, W), BF16),
        pltpu.VMEM((2, SLOTS, ROWS), BF16),
        pltpu.VMEM((SLOTS, W), BF16),
        pltpu.VMEM((T, SLOTS, W), BF16),
        pltpu.VMEM((SLOTS, 512), F32),
        pltpu.VMEM((X, SLOTS, W), BF16),
        pltpu.VMEM((Y, SLOTS, W), BF16),
        pltpu.VMEM((3, SLOTS, W), BF16),
        pltpu.VMEM((3, SLOTS, W), BF16),
        pltpu.VMEM((3, SLOTS, W), BF16),
        pltpu.VMEM((3, SLOTS, W), BF16),
        pltpu.VMEM((SLOTS, W), BF16),
        pltpu.VMEM((SLOTS, W), BF16),
        pltpu.VMEM((Z, 9, W), F32),
        pltpu.VMEM((E, 9, W), F32),
        pltpu.VMEM((E, 8, W), F32),
        pltpu.VMEM((Z, 8, W), F32),
        pltpu.VMEM((ROWS, W), F32),
        pltpu.VMEM((ROWS, W), BF16),
        pltpu.VMEM((ROWS, W), F32),
        pltpu.VMEM((2, W, W), F32),
        pltpu.VMEM((T, ROWS, W), BF16),
        pltpu.VMEM((2, SLOTS, 512), F32),
        pltpu.SemaphoreType.DMA((18,)),
        pltpu.SemaphoreType.DMA((160,)),
        pltpu.SemaphoreType.DMA((160,)),
        pltpu.SemaphoreType.DMA((9,)),
    ]
    out = jax.ShapeDtypeStruct((ROWS, W), BF16)
    return pl.pallas_call(
        kernel,
        out_shape=(out, out),
        in_specs=[hbm] * 17,
        out_specs=(hbm, hbm),
        scratch_shapes=scratch,
        compiler_params=pltpu.CompilerParams(
            collective_id=0, has_side_effects=True, vmem_limit_bytes=67043328
        ),
    )(
        queries, keys, values, gates, log_decay.reshape(2, BLOCK), out_weight,
        moe_rows, moe_gain.reshape(T, W), routes.T, route_weights.T,
        gate_proj.reshape(D, 256), up_proj.reshape(D, 256),
        down_proj.reshape(Y, X, 2, W, W), *tables(),
    )


def solution(mesh):
    torus = Mesh(mesh.devices.reshape(Z, C, Y, X), ("ep_0", "ep_1", "tp_0", "tp_1"))
    return jax.shard_map(
        on_device,
        mesh=torus,
        in_specs=(
            P(EP, TP), P(EP, TP), P(EP, TP), P(EP, TP), P(EP, TP), P(None, TP),
            P(EP, None), P(), P(EP, None), P(EP, None),
            P(EP, None, TP), P(EP, None, TP), P(EP, None, TP),
        ),
        out_specs=(P(EP, TP), P(EP, TP)),
        check_vma=False,
    )
```

```python
import jax
import jax.numpy as jnp
import numpy as np
from jax import lax
from jax.experimental import pallas as pl
from jax.experimental.pallas import tpu as pltpu
from jax.sharding import Mesh
from jax.sharding import PartitionSpec as P

MESH = pl.DeviceIdType.MESH
F32 = jnp.float32
BF16 = jnp.bfloat16
Z, C, Y, X = 16, 2, 4, 4
E = Z * C
T = Y * X
ROWS = 256
SLOTS = 2 * ROWS
CAP = SLOTS // E
D = 2048
W = 128
BLOCK = 128
CHUNKS = 4
ORDER = (
    "O0", "F0", "O1", "O2", "O3", "W0", "F1", "F2", "F3", "S0", "L0", "L1", "L2", "L3", "U0",
    "H0", "H1", "H2", "H3", "R0", "M0", "V0", "K1", "D1", "K2", "D2", "K0", "D0", "K3", "D3",
    "M1", "X1", "X2", "X0", "X3", "M2", "M3",
)
RELAY_ROWS = (1, 1, 1, 1)
RELAY_HIDDEN = (0, 0, 0, 0)
RELAY_HEADS = 1
CHUNK = SLOTS // CHUNKS
OWN = 4
EP = ("ep_0", "ep_1")
TP = ("tp_0", "tp_1")


def mm(a, b, ca=1, cb=0):
    return lax.dot_general(a, b, (((ca,), (cb,)), ((), ())), preferred_element_type=F32)


def parts_of(a, count):
    found = []
    for k in range(count):
        piece = a.astype(BF16)
        found.append(piece)
        if k + 1 < count:
            a = a - piece.astype(F32)
    return found


def silu(v):
    return v / (1.0 + jnp.exp(-v))


def chosen(relayed, onward, straight):
    act = (straight, onward)
    if relayed < 2:
        if act[relayed] is not None:
            act[relayed]()
        return
    for core in range(2):
        if act[core] is not None:
            pl.when(lax.axis_index("ep_1") == core)(act[core])


def rows_in(buf, rows):
    count = 1
    while rows % count or rows // count > buf.shape[1]:
        count += 1
    return buf.at[pl.ds(0, count), pl.ds(0, rows // count)]


class Spread:
    def __init__(self, buf, starts, n, place, relayed, send, recv):
        self.buf, self.starts, self.n, self.place = buf, starts, n, place
        self.relayed, self.send, self.recv = relayed, send, recv

    def block(self, half, dp, dq):
        y, x = self.place
        dy, dx = (dq, dp) if half == 0 else (dp, dq)
        return lax.rem(y + dy + Y, Y), lax.rem(x + dx + X, X)

    def go(self, half, k, frm, to, part=None):
        y, x = self.block(half, *frm)
        start, count = self.starts[half], self.n
        if part is not None:
            count //= 2
            start += part * count
        ref = self.buf.at[y * X + x, pl.ds(start, count)]
        ty, tx = self.block(half, *to)
        pltpu.make_async_remote_copy(
            src_ref=ref,
            dst_ref=ref,
            send_sem=self.send,
            recv_sem=self.recv(k),
            device_id={"tp_0": ty, "tp_1": tx},
            device_id_type=MESH,
        ).start()

    def across(self, j):
        def straight():
            for half in range(2):
                self.go(half, 3, (j, 0), (0, 2))

        chosen(self.relayed, None, straight)
        for to in (1, -1):
            for half in range(2):
                self.go(half, 2 if j else 1, (j, 0), (0, to))

    def own(self):
        for to in (2, -1, 1):
            for half in range(2):
                self.go(half, 0, (0, 0), (to, 0))
        self.across(0)

    def first(self):
        self.got(0, 6)
        for j in (-1, 1, 2):
            self.across(j)

    def relay(self):
        for k, blocks, js in ((1, 4, (0,)), (2, 12, (-1, 1, 2))):
            self.got(k, blocks)

            def onward(js=js):
                for j in js:
                    for half in range(2):
                        self.go(half, 3, (j, -1), (0, 1), 0)
                        self.go(half, 3, (j, 1), (0, -1), 1)

            chosen(self.relayed, onward, None)

    def rest(self):
        self.got(3, 8)

    def got(self, k, blocks):
        landed(rows_in(self.buf, blocks * self.n), self.recv(k))


def whole_copy(region, sem):
    return pltpu.make_async_remote_copy(
        src_ref=region,
        dst_ref=region,
        send_sem=sem,
        recv_sem=sem,
        device_id={"tp_1": lax.rem(lax.axis_index("tp_1") + 1, X)},
        device_id_type=MESH,
    )


def landed(region, sem):
    whole_copy(region, sem).wait_recv()


def departed(region, sem):
    whole_copy(region, sem).wait_send()


def kernel(
    q_hbm, k_hbm, v_hbm, g_hbm, ld_hbm, wo_hbm, rows_hbm, gain_hbm, routes_hbm, rw_hbm,
    wg_hbm, wu_hbm, wd_hbm, cr_hbm, sr_hbm, cb_hbm, sb_hbm,
    mix_hbm, moe_hbm,
    q_ref, k_ref, v_ref, g_ref, ld_ref, rows_ref, gain_ref, routes_ref, rw_ref,
    cr_ref, sr_ref, cb_ref, sb_ref, mix_ref, moe_ref,
    wg, wu, wo, wa, wb, wt, oh, snd, rbuf, ha, hb, pa, pb, ra, rb, eo, ret,
    sts, str_, sto, sti, ins, rotq, cum, upd, ho, psum,
    lsem, send, recv, zsem,
):
    z, c = lax.axis_index("ep_0"), lax.axis_index("ep_1")
    y, x = lax.axis_index("tp_0"), lax.axis_index("tp_1")
    e = z * C + c
    t = y * X + x

    barrier = pltpu.get_barrier_semaphore()
    wd_rows = wd_hbm
    routed = (
        (routes_hbm, routes_ref), (rows_hbm, rows_ref), (gain_hbm, gain_ref), (rw_hbm, rw_ref),
    )
    mixed = (
        (k_hbm, k_ref), (q_hbm, q_ref), (v_hbm, v_ref), (ld_hbm, ld_ref), (cr_hbm, cr_ref),
        (sr_hbm, sr_ref), (cb_hbm.at[e], cb_ref), (sb_hbm.at[e], sb_ref), (g_hbm, g_ref),
    )
    held = (
        (wg_hbm, wg), (wu_hbm, wu), (wd_rows.at[y, :, 0], wa.at[y]),
        (wd_rows.at[:, x, 1], wb.at[x]), (wo_hbm, wo),
    )
    local = [
        pltpu.make_async_copy(src, dst, lsem.at[n])
        for n, (src, dst) in enumerate(routed + mixed + held)
    ]
    routed, mixed, local = (
        local[: len(routed)], local[len(routed) : -len(held)], local[-len(held) :],
    )
    for copy in routed:
        copy.start()

    def ring_dev(d):
        j = lax.rem(e + d, E)
        return j, {"ep_0": j // C, "ep_1": lax.rem(j, C)}

    def greet(d, _):
        pl.semaphore_signal(barrier, inc=1, device_id=ring_dev(d)[1], device_id_type=MESH)
        return _

    lax.fori_loop(1, E, greet, 0)
    for s in range(1, 4):
        pl.semaphore_signal(
            barrier, inc=1, device_id={"tp_0": lax.rem(y + s, Y)}, device_id_type=MESH
        )
        pl.semaphore_signal(
            barrier, inc=1, device_id={"tp_1": lax.rem(x + s, X)}, device_id_type=MESH
        )

    for copy in mixed + local:
        copy.start()

    for copy in routed:
        copy.wait()

    slot_id = lax.broadcasted_iota(jnp.int32, (SLOTS, ROWS), 0)
    expert_of = slot_id // CAP
    place_of = (slot_id - expert_of * CAP).astype(F32)
    named = [routes_ref[k : k + 1, :] == expert_of for k in range(2)]
    either = jnp.logical_or(named[0], named[1])
    before = (
        lax.broadcasted_iota(jnp.int32, (ROWS, ROWS), 0)
        < lax.broadcasted_iota(jnp.int32, (ROWS, ROWS), 1)
    )
    rank = mm(either.astype(F32).astype(BF16), before.astype(F32).astype(BF16))
    here = rank == place_of
    for k in range(2):
        oh[k] = jnp.logical_and(named[k], here).astype(F32).astype(BF16)

    lanes = pl.ds(pl.multiple_of(t * W, W), W)
    gain_at = lax.broadcasted_iota(jnp.int32, (T, W), 0) == t
    gain = jnp.sum(jnp.where(gain_at, gain_ref[...].astype(F32), 0.0), axis=0, keepdims=True)

    def squares(r, _):
        rows = pl.ds(pl.multiple_of(r * 64, 64), 64)
        full = rows_ref[rows, :].astype(F32)
        mean = jnp.sum(full * full, axis=-1, keepdims=True) * (1.0 / D)
        mine = rows_ref[rows, lanes].astype(F32)
        normed = mine * lax.rsqrt(mean + 1e-06) * gain
        rotq[rows, :] = normed.astype(BF16)
        return _

    lax.fori_loop(0, ROWS // 64, squares, 0)
    normed = rotq[...]
    picked = mm(oh[0] + oh[1], normed)
    snd[...] = picked.astype(BF16)
    mine_at = pl.ds(pl.multiple_of(e * CAP, CAP), CAP)
    own_rows = slice(OWN * CAP, (OWN + 1) * CAP)
    rbuf[t, own_rows, :] = snd[mine_at, :]

    pl.semaphore_wait(barrier, E - 1 + 6)

    def zigzag(i, low, high):
        even = 1 - lax.rem(i, 2)
        return even * (low + i // 2) + (1 - even) * (high - i // 2)

    def source_of(n, i):
        if n == 0:
            d = zigzag(i, -4, 3)
            return d, OWN + d
        if n == 1:
            return 15 - i, 15 - i
        if n == 2:
            return 16 + i, 16 + i
        d = zigzag(i, -8, 7)
        even = 1 - lax.rem(i, 2)
        return d, 20 + d + 16 * even

    def tile(k):
        return pl.ds(pl.multiple_of(k * CAP, CAP), CAP)

    def each(n, act):
        def step(i, carry):
            act(*source_of(n, i))
            return carry

        lax.fori_loop(0, 7 if n == 0 else 8, step, 0)

    for n in range(CHUNKS):

        def dispatch(d, slot, n=n):
            j, dev = ring_dev(E - d)
            pltpu.make_async_remote_copy(
                src_ref=snd.at[tile(j)],
                dst_ref=rbuf.at[t, tile(slot)],
                send_sem=zsem.at[0],
                recv_sem=zsem.at[8 + n],
                device_id=dev,
                device_id_type=MESH,
            ).start()

        each(n, dispatch)

    def weight_copy(src, dst, sem, axis, to):
        me = y if axis == "tp_0" else x
        pltpu.make_async_remote_copy(
            src_ref=src, dst_ref=dst, send_sem=send.at[0], recv_sem=recv.at[sem],
            device_id={axis: lax.rem(me + to + 4, 4)}, device_id_type=MESH,
        ).start()

    def down_rows(side, k, part=None):
        among = pl.ds(0, 4) if part is None else pl.ds(2 * part, 2)
        return wd_rows.at[k, among, 0] if side == 0 else wd_rows.at[among, k, 1]

    wsides = ((wa, "tp_0", y), (wb, "tp_1", x))
    for side, (into, axis, me) in enumerate(wsides):
        for part, to in ((0, 1), (1, -1)):
            weight_copy(down_rows(side, lax.rem(me + 2, 4), part), wt.at[side, part], 2, axis, to)
    for side, (into, axis, me) in enumerate(wsides):
        for to in (1, -1):
            weight_copy(down_rows(side, lax.rem(me + to + 4, 4)), into.at[me], side, axis, to)

    def relay_weights():
        landed(wt, recv.at[2])
        for side, (into, axis, me) in enumerate(wsides):
            for part, to in ((0, 1), (1, -1)):
                weight_copy(
                    wt.at[side, part], into.at[lax.rem(me - to + 4, 4), pl.ds(2 * part, 2)],
                    side, axis, to,
                )

    for copy in mixed:
        copy.wait()
    cb, sb = cb_ref[...], sb_ref[...]
    cos = cb * cr_ref[...] - sb * sr_ref[...]

    def signed(first, second):
        lane = lax.broadcasted_iota(jnp.int32, first.shape, 1)
        return jnp.where(lane < W // 2, -first, second)

    sin = sb * cr_ref[...] + cb * sr_ref[...]
    sin = signed(sin, sin)

    def turned(ref):
        full = ref[...].astype(F32)
        return full * cos + pltpu.roll(full, W // 2, 1) * sin

    rq = turned(q_ref).astype(BF16)
    rotq[...] = rq
    rk = (turned(k_ref) * (W**-0.5)).astype(BF16)
    row_i = lax.broadcasted_iota(jnp.int32, (BLOCK, BLOCK), 0)
    col_i = lax.broadcasted_iota(jnp.int32, (BLOCK, BLOCK), 1)
    causal = row_i >= col_i
    tri = causal.astype(F32).astype(BF16)
    ends = []
    for b in range(2):
        rows = slice(b * BLOCK, (b + 1) * BLOCK)
        decay = jnp.broadcast_to(ld_ref[b : b + 1, :], (BLOCK, BLOCK))
        column = jnp.zeros((BLOCK, BLOCK), F32)
        line = jnp.zeros((BLOCK, BLOCK), F32)
        for piece in parts_of(decay, 3):
            column = column + mm(tri, piece, 1, 1)
            line = line + mm(piece, tri, 1, 1)
        spread = column - line
        factor = jnp.where(causal, jnp.exp(jnp.where(causal, spread, 0.0)), 0.0)
        weights = (mm(rq[rows], rk[rows], 1, 1) * factor).astype(BF16)
        values = v_ref[rows, :]
        cum[rows, :] = column
        end = column[BLOCK - 1 : BLOCK, :]
        ends.append(end)
        scaled = rk[rows].astype(F32) * jnp.exp(end - column)
        high, low = parts_of(scaled, 2)
        upd[b] = mm(high, values, 0, 0) + mm(low, values, 0, 0)
        ins[rows, :] = mm(weights, values)
    whole = jnp.exp(ends[1]) * upd[0] + upd[1]
    total = ends[0] + ends[1]
    for s in range(Z):
        sts[s, 0:8, :] = whole[s * 8 : (s + 1) * 8, :]
        sts[s, 8:9, :] = total
    upd[1] = jnp.broadcast_to(jnp.exp(ends[0]), (BLOCK, W))

    owner = c == lax.rem(z, C)
    str_[e] = sts[z]

    def give(i, carry):
        s = lax.rem(z + i, Z)

        @pl.when(jnp.logical_or(i > 0, jnp.logical_not(owner)))
        def _():
            pltpu.make_async_remote_copy(
                src_ref=sts.at[s],
                dst_ref=str_.at[e],
                send_sem=zsem.at[4],
                recv_sem=zsem.at[5],
                device_id={"ep_0": s, "ep_1": lax.rem(s, C)},
                device_id_type=MESH,
            ).start()

        return carry

    lax.fori_loop(0, Z, give, 0)

    place = (y, x)
    moe = []
    for n in range(CHUNKS):
        moe.append(
            Spread(
                rbuf, (n * CHUNK, n * CHUNK + CHUNK // 2), CHUNK // 2, place, RELAY_ROWS[n],
                send.at[1], lambda k, n=n: recv.at[3 + 4 * n + k],
            )
        )
    mix = Spread(ho, (0, BLOCK), BLOCK, place, RELAY_HEADS, send.at[2], lambda k: recv.at[31 + k])

    def rows_of(n):
        return slice(n * CHUNK, (n + 1) * CHUNK), pl.ds(n * CHUNK, CHUNK)

    def arrive(n):
        count = 7 if n == 0 else 8
        landed(rbuf.at[t, pl.ds(0, count * CAP)], zsem.at[8 + n])
        moe[n].own()

    def hidden(n):
        moe[n].rest()
        rows, at = rows_of(n)
        left = jnp.concatenate([rbuf[k, rows, :] for k in range(T)], axis=1)
        units = (silu(mm(left, wg[...])) * mm(left, wu[...])).astype(BF16)
        ha[x, rows, :] = units[:, 0:W]
        hb[y, rows, :] = units[:, W : 2 * W]
        def straight():
            for side in range(2):
                hop(n, side, 0, 2)

        chosen(RELAY_HIDDEN[n], None, straight)
        for to in (1, -1):
            for side in range(2):
                hop(n, side, 0, to)

    hsides = ((ha, "tp_1", x), (hb, "tp_0", y))

    def hop(n, side, block, to, part=None):
        buf, axis, me = hsides[side]
        at = pl.ds(n * CHUNK, CHUNK)
        if part is not None:
            at = pl.ds(n * CHUNK + part * CHUNK // 2, CHUNK // 2)
        ref = buf.at[lax.rem(me + block + 4, 4), at]
        near = block == 0 and to != 2
        pltpu.make_async_remote_copy(
            src_ref=ref, dst_ref=ref, send_sem=send.at[3],
            recv_sem=recv.at[19 + 2 * n + (0 if near else 1)],
            device_id={axis: lax.rem(me + to + 4, 4)}, device_id_type=MESH,
        ).start()

    def hop_relay(n):
        landed(rows_in(ha, 4 * CHUNK), recv.at[19 + 2 * n])

        def onward():
            for side in range(2):
                hop(n, side, -1, 1, 0)
                hop(n, side, 1, -1, 1)

        chosen(RELAY_HIDDEN[n], onward, None)

    def down(n):
        landed(rows_in(ha, 2 * CHUNK), recv.at[20 + 2 * n])
        rows, at = rows_of(n)
        for side in range(2):
            buf, weight, out, into, axis, me = (
                (ha, wa, pa, ra, "tp_0", y), (hb, wb, pb, rb, "tp_1", x),
            )[side]
            left = jnp.concatenate([buf[k, rows, :] for k in range(4)], axis=1)
            right = jnp.concatenate(
                [weight[lax.rem(me + s, 4)].reshape(4 * W, W) for s in range(4)], axis=1
            )
            whole = mm(left, right)
            for s in (2, 1, 3):
                out[s - 1, rows, :] = whole[:, s * W : (s + 1) * W].astype(BF16)
                pltpu.make_async_remote_copy(
                    src_ref=out.at[s - 1, at], dst_ref=into.at[s - 1, at],
                    send_sem=send.at[4], recv_sem=recv.at[27 + n],
                    device_id={axis: lax.rem(me + s, 4)}, device_id_type=MESH,
                ).start()
            psum[side, rows, :] = whole[:, 0:W]

    def give_back(d, slot):
        pltpu.make_async_remote_copy(
            src_ref=eo.at[tile(slot)],
            dst_ref=ret.at[mine_at],
            send_sem=zsem.at[2],
            recv_sem=zsem.at[3],
            device_id=ring_dev(E + d)[1],
            device_id_type=MESH,
        ).start()

    def finish(n):
        landed(ra.at[pl.ds(0, 3), pl.ds(0, 2 * CHUNK)], recv.at[27 + n])
        rows, _ = rows_of(n)
        summed = psum[0, rows, :] + psum[1, rows, :]
        for into in (ra, rb):
            for s in range(3):
                summed = summed + into[s, rows, :].astype(F32)
        eo[rows, :] = summed.astype(BF16)
        if n == 0:
            ret[mine_at, :] = eo[own_rows, :]
        each(n, give_back)

    def scan_states():
        @pl.when(owner)
        def _():
            landed(str_.at[pl.ds(0, E - 1)], zsem.at[5])
            current = jnp.zeros((8, W), F32)
            for j in range(E):
                sto[j] = current
                if j + 1 < E:
                    current = jnp.exp(str_[j, 8:9, :]) * current + str_[j, 0:8, :]
            sti[z] = sto[e]

            def back(i, _):
                j, dev = ring_dev(i + 1)
                pltpu.make_async_remote_copy(
                    src_ref=sto.at[j],
                    dst_ref=sti.at[z],
                    send_sem=zsem.at[6],
                    recv_sem=zsem.at[7],
                    device_id=dev,
                    device_id_type=MESH,
                ).start()
                return _

            lax.fori_loop(0, E - 1, back, 0)

    def retain():
        @pl.when(owner)
        def _():
            landed(sti.at[pl.ds(0, Z - 1)], zsem.at[7])

        @pl.when(jnp.logical_not(owner))
        def _():
            landed(sti, zsem.at[7])

        entering = sti[...].reshape(W, W)
        for b in range(2):
            rows = slice(b * BLOCK, (b + 1) * BLOCK)
            high, low = parts_of(entering, 2)
            query = rotq[rows, :]
            carried = (mm(query, high) + mm(query, low)) * jnp.exp(cum[rows, :])
            retained = ins[rows, :] + carried
            mean = jnp.sum(retained * retained, axis=-1, keepdims=True) * (1.0 / W)
            gate = g_ref[rows, :].astype(F32)
            ho[t, rows, :] = (retained * lax.rsqrt(mean + 1e-05) * silu(gate)).astype(BF16)
            entering = upd[1] * entering + upd[0]

    def weights_here(n):
        for copy in local[:2]:
            copy.wait()

    def down_weights_here(n):
        for copy in local[2:4]:
            copy.wait()
        landed(wa.at[pl.ds(0, 3)], recv.at[0])
        landed(wb.at[pl.ds(0, 3)], recv.at[1])

    steps = {
        "O": arrive,
        "F": lambda n: moe[n].first(),
        "L": lambda n: moe[n].relay(),
        "U": weights_here,
        "H": hidden,
        "K": hop_relay,
        "V": down_weights_here,
        "D": down,
        "X": finish,
        "W": lambda n: relay_weights(),
        "S": lambda n: scan_states(),
        "R": lambda n: retain(),
        "M": lambda n: (mix.own, mix.first, mix.relay, mix.rest)[n](),
    }
    for name in ORDER:
        steps[name[0]](int(name[1]))
    local[4].wait()
    heads = jnp.concatenate([ho[k] for k in range(T)], axis=1)
    mix_ref[...] = mm(heads, wo[...]).astype(BF16)
    mix_out = pltpu.make_async_copy(mix_ref, mix_hbm, lsem.at[0])
    mix_out.start()

    landed(ret.at[pl.ds(0, (E - 1) * CAP)], zsem.at[3])
    moe_out = jnp.zeros((ROWS, W), F32)
    for k in range(2):
        share = jnp.transpose(jnp.broadcast_to(rw_ref[k : k + 1, :], (W, ROWS)))
        moe_out = moe_out + mm(oh[k], ret[...], 0, 0) * share
    moe_ref[...] = moe_out.astype(BF16)
    moe_copy = pltpu.make_async_copy(moe_ref, moe_hbm, lsem.at[1])
    moe_copy.start()

    for n, region in (
        (0, rbuf.at[pl.ds(0, 8)]), (1, rbuf.at[pl.ds(0, 15)]), (2, ho.at[pl.ds(0, 15)]),
        (3, rbuf.at[pl.ds(0, 6)]), (4, rbuf.at[pl.ds(0, 6)]),
    ):
        departed(region, send.at[n])
    departed(snd.at[pl.ds(0, (E - 1) * CAP)], zsem.at[0])
    departed(eo.at[pl.ds(0, (E - 1) * CAP)], zsem.at[2])

    @pl.when(owner)
    def _():
        departed(sts.at[pl.ds(0, Z - 1)], zsem.at[4])
        departed(sto.at[pl.ds(0, E - 1)], zsem.at[6])

    @pl.when(jnp.logical_not(owner))
    def _():
        departed(sts, zsem.at[4])

    mix_out.wait()
    moe_copy.wait()


def tables():
    half = W // 2
    inverse = 10000.0 ** (-np.arange(half, dtype=np.float64) / half)
    near = np.arange(ROWS, dtype=np.float64)[:, None] * inverse[None, :]
    base = (np.arange(E, dtype=np.float64) * ROWS)[:, None] * inverse[None, :]
    both_halves = lambda a: np.concatenate([a, a], axis=1).astype(np.float32)
    return (
        both_halves(np.cos(near)),
        both_halves(np.sin(near)),
        both_halves(np.cos(base))[:, None, :],
        both_halves(np.sin(base))[:, None, :],
    )


def on_device(
    queries, keys, values, gates, log_decay, out_weight,
    moe_rows, moe_gain, routes, route_weights, gate_proj, up_proj, down_proj,
):
    hbm = pl.BlockSpec(memory_space=pltpu.HBM)
    scratch = [
        pltpu.VMEM((ROWS, W), BF16),
        pltpu.VMEM((ROWS, W), BF16),
        pltpu.VMEM((ROWS, W), BF16),
        pltpu.VMEM((ROWS, W), BF16),
        pltpu.VMEM((2, BLOCK), F32),
        pltpu.VMEM((ROWS, D), BF16),
        pltpu.VMEM((T, W), BF16),
        pltpu.VMEM((2, ROWS), jnp.int32),
        pltpu.VMEM((2, ROWS), F32),
        pltpu.VMEM((ROWS, W), F32),
        pltpu.VMEM((ROWS, W), F32),
        pltpu.VMEM((1, W), F32),
        pltpu.VMEM((1, W), F32),
        pltpu.VMEM((ROWS, W), BF16),
        pltpu.VMEM((ROWS, W), BF16),
        pltpu.VMEM((D, 256), BF16),
        pltpu.VMEM((D, 256), BF16),
        pltpu.VMEM((D, W), BF16),
        pltpu.VMEM((Y, X, W, W), BF16),
        pltpu.VMEM((X, Y, W, W), BF16),
        pltpu.VMEM((2, 2, 2, W, W), BF16),
        pltpu.VMEM((2, SLOTS, ROWS), BF16),
        pltpu.VMEM((SLOTS, W), BF16),
        pltpu.VMEM((T, SLOTS, W), BF16),
        pltpu.VMEM((X, SLOTS, W), BF16),
        pltpu.VMEM((Y, SLOTS, W), BF16),
        pltpu.VMEM((3, SLOTS, W), BF16),
        pltpu.VMEM((3, SLOTS, W), BF16),
        pltpu.VMEM((3, SLOTS, W), BF16),
        pltpu.VMEM((3, SLOTS, W), BF16),
        pltpu.VMEM((SLOTS, W), BF16),
        pltpu.VMEM((SLOTS, W), BF16),
        pltpu.VMEM((Z, 9, W), F32),
        pltpu.VMEM((E, 9, W), F32),
        pltpu.VMEM((E, 8, W), F32),
        pltpu.VMEM((Z, 8, W), F32),
        pltpu.VMEM((ROWS, W), F32),
        pltpu.VMEM((ROWS, W), BF16),
        pltpu.VMEM((ROWS, W), F32),
        pltpu.VMEM((2, W, W), F32),
        pltpu.VMEM((T, ROWS, W), BF16),
        pltpu.VMEM((2, SLOTS, W), F32),
        pltpu.SemaphoreType.DMA((18,)),
        pltpu.SemaphoreType.DMA((5,)),
        pltpu.SemaphoreType.DMA((35,)),
        pltpu.SemaphoreType.DMA((12,)),
    ]
    out = jax.ShapeDtypeStruct((ROWS, W), BF16)
    return pl.pallas_call(
        kernel,
        out_shape=(out, out),
        in_specs=[hbm] * 17,
        out_specs=(hbm, hbm),
        scratch_shapes=scratch,
        compiler_params=pltpu.CompilerParams(
            collective_id=0, has_side_effects=True, vmem_limit_bytes=67043328
        ),
    )(
        queries, keys, values, gates, log_decay.reshape(2, BLOCK), out_weight,
        moe_rows, moe_gain.reshape(T, W), routes.T, route_weights.T,
        gate_proj.reshape(D, 256), up_proj.reshape(D, 256),
        down_proj.reshape(Y, X, 2, W, W), *tables(),
    )


def solution(mesh):
    torus = Mesh(mesh.devices.reshape(Z, C, Y, X), ("ep_0", "ep_1", "tp_0", "tp_1"))
    return jax.shard_map(
        on_device,
        mesh=torus,
        in_specs=(
            P(EP, TP), P(EP, TP), P(EP, TP), P(EP, TP), P(EP, TP), P(None, TP),
            P(EP, None), P(), P(EP, None), P(EP, None),
            P(EP, None, TP), P(EP, None, TP), P(EP, None, TP),
        ),
        out_specs=(P(EP, TP), P(EP, TP)),
        check_vma=False,
    )
```

```python
import jax
import jax.numpy as jnp
import numpy as np
from jax import lax
from jax.experimental import pallas as pl
from jax.experimental.pallas import tpu as pltpu
from jax.sharding import Mesh
from jax.sharding import PartitionSpec as P

MESH = pl.DeviceIdType.MESH
F32 = jnp.float32
BF16 = jnp.bfloat16
Z, C, Y, X = 16, 2, 4, 4
E = Z * C
T = Y * X
ROWS = 256
SLOTS = 2 * ROWS
CAP = SLOTS // E
D = 2048
W = 128
BLOCK = 128
CHUNKS = 4
ORDER = (
    "O0", "O3", "G0", "F0", "O1", "O2", "W0", "F3", "F1", "F2", "L0", "S0", "L3", "L1", "L2",
    "U0", "H0", "H1", "H2", "H3", "R0", "M0", "V0", "K1", "D1", "K2", "D2", "K0", "D0", "K3",
    "D3", "X1", "M1", "X2", "X0", "X3", "M2", "M3",
)
RELAY_ROWS = (1, 1, 1, 1)
RELAY_HIDDEN = (0, 0, 0, 0)
RELAY_HEADS = 1
CHUNK = SLOTS // CHUNKS
OWN = 4
EP = ("ep_0", "ep_1")
TP = ("tp_0", "tp_1")


def mm(a, b, ca=1, cb=0):
    return lax.dot_general(a, b, (((ca,), (cb,)), ((), ())), preferred_element_type=F32)


def parts_of(a, count):
    found = []
    for k in range(count):
        piece = a.astype(BF16)
        found.append(piece)
        if k + 1 < count:
            a = a - piece.astype(F32)
    return found


def silu(v):
    return v / (1.0 + jnp.exp(-v))


def chosen(relayed, onward, straight):
    act = (straight, onward)
    if relayed < 2:
        if act[relayed] is not None:
            act[relayed]()
        return
    for core in range(2):
        if act[core] is not None:
            pl.when(lax.axis_index("ep_1") == core)(act[core])


def rows_in(buf, rows):
    count = 1
    while rows % count or rows // count > buf.shape[1]:
        count += 1
    return buf.at[pl.ds(0, count), pl.ds(0, rows // count)]


class Spread:
    def __init__(self, buf, starts, n, place, relayed, send, recv):
        self.buf, self.starts, self.n, self.place = buf, starts, n, place
        self.relayed, self.send, self.recv = relayed, send, recv

    def block(self, half, dp, dq):
        y, x = self.place
        dy, dx = (dq, dp) if half == 0 else (dp, dq)
        return lax.rem(y + dy + Y, Y), lax.rem(x + dx + X, X)

    def go(self, half, k, frm, to, part=None):
        y, x = self.block(half, *frm)
        start, count = self.starts[half], self.n
        if part is not None:
            count //= 2
            start += part * count
        ref = self.buf.at[y * X + x, pl.ds(start, count)]
        ty, tx = self.block(half, *to)
        pltpu.make_async_remote_copy(
            src_ref=ref,
            dst_ref=ref,
            send_sem=self.send,
            recv_sem=self.recv(k),
            device_id={"tp_0": ty, "tp_1": tx},
            device_id_type=MESH,
        ).start()

    def across(self, j):
        def straight():
            for half in range(2):
                self.go(half, 3, (j, 0), (0, 2))

        chosen(self.relayed, None, straight)
        for to in (1, -1):
            for half in range(2):
                self.go(half, 2 if j else 1, (j, 0), (0, to))

    def own(self):
        for to in (2, -1, 1):
            for half in range(2):
                self.go(half, 0, (0, 0), (to, 0))
        self.across(0)

    def first(self):
        self.got(0, 6)
        for j in (-1, 1, 2):
            self.across(j)

    def relay(self):
        for k, blocks, js in ((1, 4, (0,)), (2, 12, (-1, 1, 2))):
            self.got(k, blocks)

            def onward(js=js):
                for j in js:
                    for half in range(2):
                        self.go(half, 3, (j, -1), (0, 1), 0)
                        self.go(half, 3, (j, 1), (0, -1), 1)

            chosen(self.relayed, onward, None)

    def rest(self):
        self.got(3, 8)

    def got(self, k, blocks):
        landed(rows_in(self.buf, blocks * self.n), self.recv(k))


def whole_copy(region, sem):
    return pltpu.make_async_remote_copy(
        src_ref=region,
        dst_ref=region,
        send_sem=sem,
        recv_sem=sem,
        device_id={"tp_1": lax.rem(lax.axis_index("tp_1") + 1, X)},
        device_id_type=MESH,
    )


def landed(region, sem):
    whole_copy(region, sem).wait_recv()


def departed(region, sem):
    whole_copy(region, sem).wait_send()


def kernel(
    q_hbm, k_hbm, v_hbm, g_hbm, ld_hbm, wo_hbm, rows_hbm, gain_hbm, routes_hbm, rw_hbm,
    wg_hbm, wu_hbm, wd_hbm, cr_hbm, sr_hbm, cb_hbm, sb_hbm,
    mix_hbm, moe_hbm,
    q_ref, k_ref, v_ref, g_ref, ld_ref, rows_ref, gain_ref, routes_ref, rw_ref,
    cr_ref, sr_ref, cb_ref, sb_ref, mix_ref, moe_ref,
    wg, wu, wo, wa, wb, wt, oh, snd, rbuf, ha, hb, pa, pb, ra, rb, eo, ret,
    sts, str_, sto, sti, ins, rotq, cum, upd, ho, psum,
    lsem, send, recv, zsem,
):
    z, c = lax.axis_index("ep_0"), lax.axis_index("ep_1")
    y, x = lax.axis_index("tp_0"), lax.axis_index("tp_1")
    e = z * C + c
    t = y * X + x

    barrier = pltpu.get_barrier_semaphore()

    def ring_dev(d):
        j = lax.rem(e + d, E)
        return j, {"ep_0": j // C, "ep_1": lax.rem(j, C)}

    wd_rows = wd_hbm
    routed = (
        (routes_hbm, routes_ref), (rows_hbm, rows_ref), (gain_hbm, gain_ref), (rw_hbm, rw_ref),
    )
    mixed = (
        (k_hbm, k_ref), (q_hbm, q_ref), (v_hbm, v_ref), (ld_hbm, ld_ref), (cr_hbm, cr_ref),
        (sr_hbm, sr_ref), (cb_hbm.at[e], cb_ref), (sb_hbm.at[e], sb_ref), (g_hbm, g_ref),
    )
    held = (
        (wg_hbm, wg), (wu_hbm, wu), (wd_rows.at[y, :, 0], wa.at[y]),
        (wd_rows.at[:, x, 1], wb.at[x]), (wo_hbm, wo),
    )
    local = [
        pltpu.make_async_copy(src, dst, lsem.at[n])
        for n, (src, dst) in enumerate(routed + mixed + held)
    ]
    routed, mixed, local = (
        local[: len(routed)], local[len(routed) : -len(held)], local[-len(held) :],
    )
    for copy in routed:
        copy.start()

    def greet(d):
        pl.semaphore_signal(barrier, inc=1, device_id=ring_dev(d)[1], device_id_type=MESH)

    for d in sorted(range(1, E), key=lambda d: -min(d, E - d)):
        greet(d)
    for s in range(1, 4):
        pl.semaphore_signal(
            barrier, inc=1, device_id={"tp_0": lax.rem(y + s, Y)}, device_id_type=MESH
        )
        pl.semaphore_signal(
            barrier, inc=1, device_id={"tp_1": lax.rem(x + s, X)}, device_id_type=MESH
        )

    for copy in mixed + local:
        copy.start()

    for copy in routed:
        copy.wait()

    slot_id = lax.broadcasted_iota(jnp.int32, (SLOTS, ROWS), 0)
    expert_of = slot_id // CAP
    place_of = (slot_id - expert_of * CAP).astype(F32)
    named = [routes_ref[k : k + 1, :] == expert_of for k in range(2)]
    either = jnp.logical_or(named[0], named[1])
    before = (
        lax.broadcasted_iota(jnp.int32, (ROWS, ROWS), 0)
        < lax.broadcasted_iota(jnp.int32, (ROWS, ROWS), 1)
    )
    rank = mm(either.astype(F32).astype(BF16), before.astype(F32).astype(BF16))
    here = rank == place_of
    for k in range(2):
        oh[k] = jnp.logical_and(named[k], here).astype(F32).astype(BF16)

    lanes = pl.ds(pl.multiple_of(t * W, W), W)
    gain_at = lax.broadcasted_iota(jnp.int32, (T, W), 0) == t
    gain = jnp.sum(jnp.where(gain_at, gain_ref[...].astype(F32), 0.0), axis=0, keepdims=True)

    def squares(r, _):
        rows = pl.ds(pl.multiple_of(r * 64, 64), 64)
        full = rows_ref[rows, :].astype(F32)
        mean = jnp.sum(full * full, axis=-1, keepdims=True) * (1.0 / D)
        mine = rows_ref[rows, lanes].astype(F32)
        normed = mine * lax.rsqrt(mean + 1e-06) * gain
        rotq[rows, :] = normed.astype(BF16)
        return _

    lax.fori_loop(0, ROWS // 64, squares, 0)
    normed = rotq[...]
    picked = mm(oh[0] + oh[1], normed)
    snd[...] = picked.astype(BF16)
    mine_at = pl.ds(pl.multiple_of(e * CAP, CAP), CAP)
    own_rows = slice(OWN * CAP, (OWN + 1) * CAP)
    rbuf[t, own_rows, :] = snd[mine_at, :]

    pl.semaphore_wait(barrier, E - 1 + 6)

    def zigzag(i, low, high):
        even = 1 - lax.rem(i, 2)
        return even * (low + i // 2) + (1 - even) * (high - i // 2)

    def source_of(n, i):
        if n == 0:
            d = zigzag(i, -4, 3)
            return d, OWN + d
        if n == 1:
            return 15 - i, 15 - i
        if n == 2:
            return 16 + i, 16 + i
        d = zigzag(i, -8, 7)
        even = 1 - lax.rem(i, 2)
        return d, 20 + d + 16 * even

    def tile(k):
        return pl.ds(pl.multiple_of(k * CAP, CAP), CAP)

    def each(n, act):
        def step(i, carry):
            act(*source_of(n, i))
            return carry

        lax.fori_loop(0, 7 if n == 0 else 8, step, 0)

    for n in (0, 3, 1, 2):

        def dispatch(d, slot, n=n):
            j, dev = ring_dev(E - d)
            pltpu.make_async_remote_copy(
                src_ref=snd.at[tile(j)],
                dst_ref=rbuf.at[t, tile(slot)],
                send_sem=zsem.at[0],
                recv_sem=zsem.at[8 + n],
                device_id=dev,
                device_id_type=MESH,
            ).start()

        each(n, dispatch)

    def weight_copy(src, dst, sem, axis, to):
        me = y if axis == "tp_0" else x
        pltpu.make_async_remote_copy(
            src_ref=src, dst_ref=dst, send_sem=send.at[0], recv_sem=recv.at[sem],
            device_id={axis: lax.rem(me + to + 4, 4)}, device_id_type=MESH,
        ).start()

    def down_rows(side, k, part=None):
        among = pl.ds(0, 4) if part is None else pl.ds(2 * part, 2)
        return wd_rows.at[k, among, 0] if side == 0 else wd_rows.at[among, k, 1]

    wsides = ((wa, "tp_0", y), (wb, "tp_1", x))
    for side, (into, axis, me) in enumerate(wsides):
        for part, to in ((0, 1), (1, -1)):
            weight_copy(down_rows(side, lax.rem(me + 2, 4), part), wt.at[side, part], 2, axis, to)
    for side, (into, axis, me) in enumerate(wsides):
        for to in (1, -1):
            weight_copy(down_rows(side, lax.rem(me + to + 4, 4)), into.at[me], side, axis, to)

    def relay_weights():
        landed(wt, recv.at[2])
        for side, (into, axis, me) in enumerate(wsides):
            for part, to in ((0, 1), (1, -1)):
                weight_copy(
                    wt.at[side, part], into.at[lax.rem(me - to + 4, 4), pl.ds(2 * part, 2)],
                    side, axis, to,
                )

    for copy in mixed:
        copy.wait()
    cb, sb = cb_ref[...], sb_ref[...]
    cos = cb * cr_ref[...] - sb * sr_ref[...]

    def signed(first, second):
        lane = lax.broadcasted_iota(jnp.int32, first.shape, 1)
        return jnp.where(lane < W // 2, -first, second)

    sin = sb * cr_ref[...] + cb * sr_ref[...]
    sin = signed(sin, sin)

    def turned(ref):
        full = ref[...].astype(F32)
        return full * cos + pltpu.roll(full, W // 2, 1) * sin

    rq = turned(q_ref).astype(BF16)
    rotq[...] = rq
    rk = (turned(k_ref) * (W**-0.5)).astype(BF16)
    row_i = lax.broadcasted_iota(jnp.int32, (BLOCK, BLOCK), 0)
    col_i = lax.broadcasted_iota(jnp.int32, (BLOCK, BLOCK), 1)
    causal = row_i >= col_i
    tri = causal.astype(F32).astype(BF16)
    ends = []
    for b in range(2):
        rows = slice(b * BLOCK, (b + 1) * BLOCK)
        decay = jnp.broadcast_to(ld_ref[b : b + 1, :], (BLOCK, BLOCK))
        column = jnp.zeros((BLOCK, BLOCK), F32)
        line = jnp.zeros((BLOCK, BLOCK), F32)
        for piece in parts_of(decay, 3):
            column = column + mm(tri, piece, 1, 1)
            line = line + mm(piece, tri, 1, 1)
        spread = column - line
        factor = jnp.where(causal, jnp.exp(jnp.where(causal, spread, 0.0)), 0.0)
        weights = (mm(rq[rows], rk[rows], 1, 1) * factor).astype(BF16)
        values = v_ref[rows, :]
        cum[rows, :] = column
        end = column[BLOCK - 1 : BLOCK, :]
        ends.append(end)
        scaled = rk[rows].astype(F32) * jnp.exp(end - column)
        high, low = parts_of(scaled, 2)
        upd[b] = mm(high, values, 0, 0) + mm(low, values, 0, 0)
        ins[rows, :] = mm(weights, values)
    whole = jnp.exp(ends[1]) * upd[0] + upd[1]
    total = ends[0] + ends[1]
    for s in range(Z):
        sts[s, 0:8, :] = whole[s * 8 : (s + 1) * 8, :]
        sts[s, 8:9, :] = total
    upd[1] = jnp.broadcast_to(jnp.exp(ends[0]), (BLOCK, W))

    owner = c == lax.rem(z, C)
    str_[e] = sts[z]

    def give(i, carry):
        s = lax.rem(z + i, Z)

        @pl.when(jnp.logical_or(i > 0, jnp.logical_not(owner)))
        def _():
            pltpu.make_async_remote_copy(
                src_ref=sts.at[s],
                dst_ref=str_.at[e],
                send_sem=zsem.at[4],
                recv_sem=zsem.at[5],
                device_id={"ep_0": s, "ep_1": lax.rem(s, C)},
                device_id_type=MESH,
            ).start()

        return carry

    def give_states():
        lax.fori_loop(0, Z, give, 0)

    place = (y, x)
    moe = []
    for n in range(CHUNKS):
        moe.append(
            Spread(
                rbuf, (n * CHUNK, n * CHUNK + CHUNK // 2), CHUNK // 2, place, RELAY_ROWS[n],
                send.at[1], lambda k, n=n: recv.at[3 + 4 * n + k],
            )
        )
    mix = Spread(ho, (0, BLOCK), BLOCK, place, RELAY_HEADS, send.at[2], lambda k: recv.at[31 + k])

    def rows_of(n):
        return slice(n * CHUNK, (n + 1) * CHUNK), pl.ds(n * CHUNK, CHUNK)

    def arrive(n):
        count = 7 if n == 0 else 8
        landed(rbuf.at[t, pl.ds(0, count * CAP)], zsem.at[8 + n])
        moe[n].own()

    def hidden(n):
        moe[n].rest()
        rows, at = rows_of(n)
        left = jnp.concatenate([rbuf[k, rows, :] for k in range(T)], axis=1)
        units = (silu(mm(left, wg[...])) * mm(left, wu[...])).astype(BF16)
        ha[x, rows, :] = units[:, 0:W]
        hb[y, rows, :] = units[:, W : 2 * W]
        def straight():
            for side in range(2):
                hop(n, side, 0, 2)

        chosen(RELAY_HIDDEN[n], None, straight)
        for to in (1, -1):
            for side in range(2):
                hop(n, side, 0, to)

    hsides = ((ha, "tp_1", x), (hb, "tp_0", y))

    def hop(n, side, block, to, part=None):
        buf, axis, me = hsides[side]
        at = pl.ds(n * CHUNK, CHUNK)
        if part is not None:
            at = pl.ds(n * CHUNK + part * CHUNK // 2, CHUNK // 2)
        ref = buf.at[lax.rem(me + block + 4, 4), at]
        near = block == 0 and to != 2
        pltpu.make_async_remote_copy(
            src_ref=ref, dst_ref=ref, send_sem=send.at[3],
            recv_sem=recv.at[19 + 2 * n + (0 if near else 1)],
            device_id={axis: lax.rem(me + to + 4, 4)}, device_id_type=MESH,
        ).start()

    def hop_relay(n):
        landed(rows_in(ha, 4 * CHUNK), recv.at[19 + 2 * n])

        def onward():
            for side in range(2):
                hop(n, side, -1, 1, 0)
                hop(n, side, 1, -1, 1)

        chosen(RELAY_HIDDEN[n], onward, None)

    def down(n):
        landed(rows_in(ha, 2 * CHUNK), recv.at[20 + 2 * n])
        rows, at = rows_of(n)
        for side in range(2):
            buf, weight, out, into, axis, me = (
                (ha, wa, pa, ra, "tp_0", y), (hb, wb, pb, rb, "tp_1", x),
            )[side]
            left = jnp.concatenate([buf[k, rows, :] for k in range(4)], axis=1)
            right = jnp.concatenate(
                [weight[lax.rem(me + s, 4)].reshape(4 * W, W) for s in range(4)], axis=1
            )
            whole = mm(left, right)
            for s in (2, 1, 3):
                out[s - 1, rows, :] = whole[:, s * W : (s + 1) * W].astype(BF16)
                pltpu.make_async_remote_copy(
                    src_ref=out.at[s - 1, at], dst_ref=into.at[s - 1, at],
                    send_sem=send.at[4], recv_sem=recv.at[27 + n],
                    device_id={axis: lax.rem(me + s, 4)}, device_id_type=MESH,
                ).start()
            psum[side, rows, :] = whole[:, 0:W]

    def give_back(d, slot):
        pltpu.make_async_remote_copy(
            src_ref=eo.at[tile(slot)],
            dst_ref=ret.at[mine_at],
            send_sem=zsem.at[2],
            recv_sem=zsem.at[3],
            device_id=ring_dev(E + d)[1],
            device_id_type=MESH,
        ).start()

    def finish(n):
        landed(ra.at[pl.ds(0, 3), pl.ds(0, 2 * CHUNK)], recv.at[27 + n])
        rows, _ = rows_of(n)
        summed = psum[0, rows, :] + psum[1, rows, :]
        for into in (ra, rb):
            for s in range(3):
                summed = summed + into[s, rows, :].astype(F32)
        eo[rows, :] = summed.astype(BF16)
        if n == 0:
            ret[mine_at, :] = eo[own_rows, :]
        each(n, give_back)

    def scan_states():
        @pl.when(owner)
        def _():
            landed(str_.at[pl.ds(0, E - 1)], zsem.at[5])
            current = jnp.zeros((8, W), F32)
            for j in range(E):
                sto[j] = current
                if j + 1 < E:
                    current = jnp.exp(str_[j, 8:9, :]) * current + str_[j, 0:8, :]
            sti[z] = sto[e]

            def back(i, _):
                j, dev = ring_dev(i + 1)
                pltpu.make_async_remote_copy(
                    src_ref=sto.at[j],
                    dst_ref=sti.at[z],
                    send_sem=zsem.at[6],
                    recv_sem=zsem.at[7],
                    device_id=dev,
                    device_id_type=MESH,
                ).start()
                return _

            lax.fori_loop(0, E - 1, back, 0)

    def retain():
        @pl.when(owner)
        def _():
            landed(sti.at[pl.ds(0, Z - 1)], zsem.at[7])

        @pl.when(jnp.logical_not(owner))
        def _():
            landed(sti, zsem.at[7])

        entering = sti[...].reshape(W, W)
        for b in range(2):
            rows = slice(b * BLOCK, (b + 1) * BLOCK)
            high, low = parts_of(entering, 2)
            query = rotq[rows, :]
            carried = (mm(query, high) + mm(query, low)) * jnp.exp(cum[rows, :])
            retained = ins[rows, :] + carried
            mean = jnp.sum(retained * retained, axis=-1, keepdims=True) * (1.0 / W)
            gate = g_ref[rows, :].astype(F32)
            ho[t, rows, :] = (retained * lax.rsqrt(mean + 1e-05) * silu(gate)).astype(BF16)
            entering = upd[1] * entering + upd[0]

    def weights_here(n):
        for copy in local[:2]:
            copy.wait()

    def down_weights_here(n):
        for copy in local[2:4]:
            copy.wait()
        landed(wa.at[pl.ds(0, 3)], recv.at[0])
        landed(wb.at[pl.ds(0, 3)], recv.at[1])

    steps = {
        "O": arrive,
        "F": lambda n: moe[n].first(),
        "L": lambda n: moe[n].relay(),
        "U": weights_here,
        "H": hidden,
        "K": hop_relay,
        "V": down_weights_here,
        "D": down,
        "X": finish,
        "W": lambda n: relay_weights(),
        "G": lambda n: give_states(),
        "S": lambda n: scan_states(),
        "R": lambda n: retain(),
        "M": lambda n: (mix.own, mix.first, mix.relay, mix.rest)[n](),
    }
    for name in ORDER:
        steps[name[0]](int(name[1]))
    local[4].wait()
    heads = jnp.concatenate([ho[k] for k in range(T)], axis=1)
    mix_ref[...] = mm(heads, wo[...]).astype(BF16)
    mix_out = pltpu.make_async_copy(mix_ref, mix_hbm, lsem.at[0])
    mix_out.start()

    landed(ret.at[pl.ds(0, (E - 1) * CAP)], zsem.at[3])
    moe_out = jnp.zeros((ROWS, W), F32)
    for k in range(2):
        share = jnp.transpose(jnp.broadcast_to(rw_ref[k : k + 1, :], (W, ROWS)))
        moe_out = moe_out + mm(oh[k], ret[...], 0, 0) * share
    moe_ref[...] = moe_out.astype(BF16)
    moe_copy = pltpu.make_async_copy(moe_ref, moe_hbm, lsem.at[1])
    moe_copy.start()

    for n, region in (
        (0, rbuf.at[pl.ds(0, 8)]), (1, rbuf.at[pl.ds(0, 15)]), (2, ho.at[pl.ds(0, 15)]),
        (3, rbuf.at[pl.ds(0, 6)]), (4, rbuf.at[pl.ds(0, 6)]),
    ):
        departed(region, send.at[n])
    departed(snd.at[pl.ds(0, (E - 1) * CAP)], zsem.at[0])
    departed(eo.at[pl.ds(0, (E - 1) * CAP)], zsem.at[2])

    @pl.when(owner)
    def _():
        departed(sts.at[pl.ds(0, Z - 1)], zsem.at[4])
        departed(sto.at[pl.ds(0, E - 1)], zsem.at[6])

    @pl.when(jnp.logical_not(owner))
    def _():
        departed(sts, zsem.at[4])

    mix_out.wait()
    moe_copy.wait()


def tables():
    half = W // 2
    inverse = 10000.0 ** (-np.arange(half, dtype=np.float64) / half)
    near = np.arange(ROWS, dtype=np.float64)[:, None] * inverse[None, :]
    base = (np.arange(E, dtype=np.float64) * ROWS)[:, None] * inverse[None, :]
    both_halves = lambda a: np.concatenate([a, a], axis=1).astype(np.float32)
    return (
        both_halves(np.cos(near)),
        both_halves(np.sin(near)),
        both_halves(np.cos(base))[:, None, :],
        both_halves(np.sin(base))[:, None, :],
    )


def on_device(
    queries, keys, values, gates, log_decay, out_weight,
    moe_rows, moe_gain, routes, route_weights, gate_proj, up_proj, down_proj,
):
    hbm = pl.BlockSpec(memory_space=pltpu.HBM)
    scratch = [
        pltpu.VMEM((ROWS, W), BF16),
        pltpu.VMEM((ROWS, W), BF16),
        pltpu.VMEM((ROWS, W), BF16),
        pltpu.VMEM((ROWS, W), BF16),
        pltpu.VMEM((2, BLOCK), F32),
        pltpu.VMEM((ROWS, D), BF16),
        pltpu.VMEM((T, W), BF16),
        pltpu.VMEM((2, ROWS), jnp.int32),
        pltpu.VMEM((2, ROWS), F32),
        pltpu.VMEM((ROWS, W), F32),
        pltpu.VMEM((ROWS, W), F32),
        pltpu.VMEM((1, W), F32),
        pltpu.VMEM((1, W), F32),
        pltpu.VMEM((ROWS, W), BF16),
        pltpu.VMEM((ROWS, W), BF16),
        pltpu.VMEM((D, 256), BF16),
        pltpu.VMEM((D, 256), BF16),
        pltpu.VMEM((D, W), BF16),
        pltpu.VMEM((Y, X, W, W), BF16),
        pltpu.VMEM((X, Y, W, W), BF16),
        pltpu.VMEM((2, 2, 2, W, W), BF16),
        pltpu.VMEM((2, SLOTS, ROWS), BF16),
        pltpu.VMEM((SLOTS, W), BF16),
        pltpu.VMEM((T, SLOTS, W), BF16),
        pltpu.VMEM((X, SLOTS, W), BF16),
        pltpu.VMEM((Y, SLOTS, W), BF16),
        pltpu.VMEM((3, SLOTS, W), BF16),
        pltpu.VMEM((3, SLOTS, W), BF16),
        pltpu.VMEM((3, SLOTS, W), BF16),
        pltpu.VMEM((3, SLOTS, W), BF16),
        pltpu.VMEM((SLOTS, W), BF16),
        pltpu.VMEM((SLOTS, W), BF16),
        pltpu.VMEM((Z, 9, W), F32),
        pltpu.VMEM((E, 9, W), F32),
        pltpu.VMEM((E, 8, W), F32),
        pltpu.VMEM((Z, 8, W), F32),
        pltpu.VMEM((ROWS, W), F32),
        pltpu.VMEM((ROWS, W), BF16),
        pltpu.VMEM((ROWS, W), F32),
        pltpu.VMEM((2, W, W), F32),
        pltpu.VMEM((T, ROWS, W), BF16),
        pltpu.VMEM((2, SLOTS, W), F32),
        pltpu.SemaphoreType.DMA((18,)),
        pltpu.SemaphoreType.DMA((5,)),
        pltpu.SemaphoreType.DMA((35,)),
        pltpu.SemaphoreType.DMA((12,)),
    ]
    out = jax.ShapeDtypeStruct((ROWS, W), BF16)
    return pl.pallas_call(
        kernel,
        out_shape=(out, out),
        in_specs=[hbm] * 17,
        out_specs=(hbm, hbm),
        scratch_shapes=scratch,
        compiler_params=pltpu.CompilerParams(
            collective_id=0, has_side_effects=True, vmem_limit_bytes=67043328
        ),
    )(
        queries, keys, values, gates, log_decay.reshape(2, BLOCK), out_weight,
        moe_rows, moe_gain.reshape(T, W), routes.T, route_weights.T,
        gate_proj.reshape(D, 256), up_proj.reshape(D, 256),
        down_proj.reshape(Y, X, 2, W, W), *tables(),
    )


def solution(mesh):
    torus = Mesh(mesh.devices.reshape(Z, C, Y, X), ("ep_0", "ep_1", "tp_0", "tp_1"))
    return jax.shard_map(
        on_device,
        mesh=torus,
        in_specs=(
            P(EP, TP), P(EP, TP), P(EP, TP), P(EP, TP), P(EP, TP), P(None, TP),
            P(EP, None), P(), P(EP, None), P(EP, None),
            P(EP, None, TP), P(EP, None, TP), P(EP, None, TP),
        ),
        out_specs=(P(EP, TP), P(EP, TP)),
        check_vma=False,
    )
```

```python
import jax
import jax.numpy as jnp
import numpy as np
from jax import lax
from jax.experimental import pallas as pl
from jax.experimental.pallas import tpu as pltpu
from jax.sharding import Mesh
from jax.sharding import PartitionSpec as P

MESH = pl.DeviceIdType.MESH
F32 = jnp.float32
BF16 = jnp.bfloat16
Z, C, Y, X = 16, 2, 4, 4
E = Z * C
T = Y * X
ROWS = 256
SLOTS = 2 * ROWS
CAP = SLOTS // E
D = 2048
W = 128
BLOCK = 128
CHUNKS = 4
ORDER = (
    "W0", "O0", "O3", "G0", "F0", "O1", "O2", "F3", "F1", "F2", "L0", "S0", "L3", "L1", "L2",
    "U0", "H0", "H1", "H2", "H3", "R0", "M0", "V0", "K1", "D1", "K2", "D2", "K0", "D0", "K3",
    "D3", "X1", "M1", "X2", "X0", "X3", "M2", "M3",
)
RELAY_ROWS = (1, 1, 1, 1)
RELAY_HIDDEN = (0, 0, 0, 0)
RELAY_HEADS = 1
CHUNK = SLOTS // CHUNKS
OWN = 4
EP = ("ep_0", "ep_1")
TP = ("tp_0", "tp_1")


def mm(a, b, ca=1, cb=0):
    return lax.dot_general(a, b, (((ca,), (cb,)), ((), ())), preferred_element_type=F32)


def parts_of(a, count):
    found = []
    for k in range(count):
        piece = a.astype(BF16)
        found.append(piece)
        if k + 1 < count:
            a = a - piece.astype(F32)
    return found


def silu(v):
    return v / (1.0 + jnp.exp(-v))


def chosen(relayed, onward, straight):
    act = (straight, onward)
    if relayed < 2:
        if act[relayed] is not None:
            act[relayed]()
        return
    for core in range(2):
        if act[core] is not None:
            pl.when(lax.axis_index("ep_1") == core)(act[core])


def rows_in(buf, rows):
    count = 1
    while rows % count or rows // count > buf.shape[1]:
        count += 1
    return buf.at[pl.ds(0, count), pl.ds(0, rows // count)]


class Spread:
    def __init__(self, buf, starts, n, place, relayed, send, recv):
        self.buf, self.starts, self.n, self.place = buf, starts, n, place
        self.relayed, self.send, self.recv = relayed, send, recv

    def block(self, half, dp, dq):
        y, x = self.place
        dy, dx = (dq, dp) if half == 0 else (dp, dq)
        return lax.rem(y + dy + Y, Y), lax.rem(x + dx + X, X)

    def go(self, half, k, frm, to, part=None):
        y, x = self.block(half, *frm)
        start, count = self.starts[half], self.n
        if part is not None:
            count //= 2
            start += part * count
        ref = self.buf.at[y * X + x, pl.ds(start, count)]
        ty, tx = self.block(half, *to)
        pltpu.make_async_remote_copy(
            src_ref=ref,
            dst_ref=ref,
            send_sem=self.send,
            recv_sem=self.recv(k),
            device_id={"tp_0": ty, "tp_1": tx},
            device_id_type=MESH,
        ).start()

    def across(self, j):
        def straight():
            for half in range(2):
                self.go(half, 3, (j, 0), (0, 2))

        chosen(self.relayed, None, straight)
        for to in (1, -1):
            for half in range(2):
                self.go(half, 2 if j else 1, (j, 0), (0, to))

    def own(self):
        for to in (2, -1, 1):
            for half in range(2):
                self.go(half, 0, (0, 0), (to, 0))
        self.across(0)

    def first(self):
        self.got(0, 6)
        for j in (-1, 1, 2):
            self.across(j)

    def relay(self):
        for k, blocks, js in ((1, 4, (0,)), (2, 12, (-1, 1, 2))):
            self.got(k, blocks)

            def onward(js=js):
                for j in js:
                    for half in range(2):
                        self.go(half, 3, (j, -1), (0, 1), 0)
                        self.go(half, 3, (j, 1), (0, -1), 1)

            chosen(self.relayed, onward, None)

    def rest(self):
        self.got(3, 8)

    def got(self, k, blocks):
        landed(rows_in(self.buf, blocks * self.n), self.recv(k))


def whole_copy(region, sem):
    return pltpu.make_async_remote_copy(
        src_ref=region,
        dst_ref=region,
        send_sem=sem,
        recv_sem=sem,
        device_id={"tp_1": lax.rem(lax.axis_index("tp_1") + 1, X)},
        device_id_type=MESH,
    )


def landed(region, sem):
    whole_copy(region, sem).wait_recv()


def departed(region, sem):
    whole_copy(region, sem).wait_send()


def kernel(
    q_hbm, k_hbm, v_hbm, g_hbm, ld_hbm, wo_hbm, rows_hbm, gain_hbm, routes_hbm, rw_hbm,
    wg_hbm, wu_hbm, wd_hbm, cr_hbm, sr_hbm, cb_hbm, sb_hbm,
    out_hbm,
    q_ref, k_ref, v_ref, g_ref, ld_ref, rows_ref, gain_ref, routes_ref, rw_ref,
    cr_ref, sr_ref, cb_ref, sb_ref, mix_ref, moe_ref,
    wg, wu, wo, wa, wb, oh, snd, rbuf, ha, hb, pa, pb, ra, rb, eo, ret,
    sts, str_, sto, sti, ins, rotq, cum, upd, ho, psum,
    lsem, send, recv, zsem,
):
    z, c = lax.axis_index("ep_0"), lax.axis_index("ep_1")
    y, x = lax.axis_index("tp_0"), lax.axis_index("tp_1")
    e = z * C + c
    t = y * X + x

    barrier = pltpu.get_barrier_semaphore()

    def ring_dev(d):
        j = lax.rem(e + d, E)
        return j, {"ep_0": j // C, "ep_1": lax.rem(j, C)}

    wd_rows = wd_hbm
    routed = (
        (routes_hbm, routes_ref), (rows_hbm, rows_ref), (gain_hbm, gain_ref), (rw_hbm, rw_ref),
    )
    mixed = (
        (k_hbm, k_ref), (q_hbm, q_ref), (v_hbm, v_ref), (ld_hbm, ld_ref), (cr_hbm, cr_ref),
        (sr_hbm, sr_ref), (cb_hbm.at[e], cb_ref), (sb_hbm.at[e], sb_ref), (g_hbm, g_ref),
    )
    held = (
        (wg_hbm, wg), (wu_hbm, wu), (wd_rows.at[y, :, 0], wa.at[y]),
        (wd_rows.at[:, x, 1], wb.at[x]), (wo_hbm, wo),
    )
    local = [
        pltpu.make_async_copy(src, dst, lsem.at[n])
        for n, (src, dst) in enumerate(routed + mixed + held)
    ]
    routed, mixed, local = (
        local[: len(routed)], local[len(routed) : -len(held)], local[-len(held) :],
    )
    for copy in routed:
        copy.start()

    def greet(d):
        pl.semaphore_signal(barrier, inc=1, device_id=ring_dev(d)[1], device_id_type=MESH)

    for d in sorted(range(1, E), key=lambda d: -min(d, E - d)):
        greet(d)
    for s in range(1, 4):
        pl.semaphore_signal(
            barrier, inc=1, device_id={"tp_0": lax.rem(y + s, Y)}, device_id_type=MESH
        )
        pl.semaphore_signal(
            barrier, inc=1, device_id={"tp_1": lax.rem(x + s, X)}, device_id_type=MESH
        )

    for copy in mixed + local:
        copy.start()

    for copy in routed:
        copy.wait()

    slot_id = lax.broadcasted_iota(jnp.int32, (SLOTS, ROWS), 0)
    expert_of = slot_id // CAP
    place_of = (slot_id - expert_of * CAP).astype(F32)
    named = [routes_ref[k : k + 1, :] == expert_of for k in range(2)]
    either = jnp.logical_or(named[0], named[1])
    before = (
        lax.broadcasted_iota(jnp.int32, (ROWS, ROWS), 0)
        < lax.broadcasted_iota(jnp.int32, (ROWS, ROWS), 1)
    )
    rank = mm(either.astype(F32).astype(BF16), before.astype(F32).astype(BF16))
    here = rank == place_of
    for k in range(2):
        oh[k] = jnp.logical_and(named[k], here).astype(F32).astype(BF16)

    lanes = pl.ds(pl.multiple_of(t * W, W), W)
    gain_at = lax.broadcasted_iota(jnp.int32, (T, W), 0) == t
    gain = jnp.sum(jnp.where(gain_at, gain_ref[...].astype(F32), 0.0), axis=0, keepdims=True)

    def squares(r, _):
        rows = pl.ds(pl.multiple_of(r * 64, 64), 64)
        full = rows_ref[rows, :].astype(F32)
        mean = jnp.sum(full * full, axis=-1, keepdims=True) * (1.0 / D)
        mine = rows_ref[rows, lanes].astype(F32)
        normed = mine * lax.rsqrt(mean + 1e-06) * gain
        rotq[rows, :] = normed.astype(BF16)
        return _

    lax.fori_loop(0, ROWS // 64, squares, 0)
    normed = rotq[...]
    picked = mm(oh[0] + oh[1], normed)
    snd[...] = picked.astype(BF16)
    mine_at = pl.ds(pl.multiple_of(e * CAP, CAP), CAP)
    own_rows = slice(OWN * CAP, (OWN + 1) * CAP)
    rbuf[t, own_rows, :] = snd[mine_at, :]

    pl.semaphore_wait(barrier, E - 1 + 6)

    def zigzag(i, low, high):
        even = 1 - lax.rem(i, 2)
        return even * (low + i // 2) + (1 - even) * (high - i // 2)

    def source_of(n, i):
        if n == 0:
            d = zigzag(i, -4, 3)
            return d, OWN + d
        if n == 1:
            return 15 - i, 15 - i
        if n == 2:
            return 16 + i, 16 + i
        d = zigzag(i, -8, 7)
        even = 1 - lax.rem(i, 2)
        return d, 20 + d + 16 * even

    def tile(k):
        return pl.ds(pl.multiple_of(k * CAP, CAP), CAP)

    def each(n, act):
        def step(i, carry):
            act(*source_of(n, i))
            return carry

        lax.fori_loop(0, 7 if n == 0 else 8, step, 0)

    for n in (0, 3, 1, 2):

        def dispatch(d, slot, n=n):
            j, dev = ring_dev(E - d)
            pltpu.make_async_remote_copy(
                src_ref=snd.at[tile(j)],
                dst_ref=rbuf.at[t, tile(slot)],
                send_sem=zsem.at[0],
                recv_sem=zsem.at[8 + n],
                device_id=dev,
                device_id_type=MESH,
            ).start()

        each(n, dispatch)

    def weight_copy(src, dst, sem, axis, to):
        me = y if axis == "tp_0" else x
        pltpu.make_async_remote_copy(
            src_ref=src, dst_ref=dst, send_sem=send.at[0], recv_sem=recv.at[sem],
            device_id={axis: lax.rem(me + to + 4, 4)}, device_id_type=MESH,
        ).start()

    wsides = ((wa, "tp_0", y), (wb, "tp_1", x))

    def send_weights(*shifts):
        for side, (into, axis, me) in enumerate(wsides):
            for to in shifts:
                k = lax.rem(me + to + 4, 4)
                rows = wd_rows.at[k, :, 0] if side == 0 else wd_rows.at[:, k, 1]
                weight_copy(rows, into.at[me], side, axis, to)

    send_weights(1, -1)

    for copy in mixed:
        copy.wait()
    cb, sb = cb_ref[...], sb_ref[...]
    cos = cb * cr_ref[...] - sb * sr_ref[...]

    def signed(first, second):
        lane = lax.broadcasted_iota(jnp.int32, first.shape, 1)
        return jnp.where(lane < W // 2, -first, second)

    sin = sb * cr_ref[...] + cb * sr_ref[...]
    sin = signed(sin, sin)

    def turned(ref):
        full = ref[...].astype(F32)
        return full * cos + pltpu.roll(full, W // 2, 1) * sin

    rq = turned(q_ref).astype(BF16)
    rotq[...] = rq
    rk = (turned(k_ref) * (W**-0.5)).astype(BF16)
    row_i = lax.broadcasted_iota(jnp.int32, (BLOCK, BLOCK), 0)
    col_i = lax.broadcasted_iota(jnp.int32, (BLOCK, BLOCK), 1)
    causal = row_i >= col_i
    tri = causal.astype(F32).astype(BF16)
    ends = []
    for b in range(2):
        rows = slice(b * BLOCK, (b + 1) * BLOCK)
        decay = jnp.broadcast_to(ld_ref[b : b + 1, :], (BLOCK, BLOCK))
        column = jnp.zeros((BLOCK, BLOCK), F32)
        line = jnp.zeros((BLOCK, BLOCK), F32)
        for piece in parts_of(decay, 3):
            column = column + mm(tri, piece, 1, 1)
            line = line + mm(piece, tri, 1, 1)
        spread = column - line
        factor = jnp.where(causal, jnp.exp(jnp.where(causal, spread, 0.0)), 0.0)
        weights = (mm(rq[rows], rk[rows], 1, 1) * factor).astype(BF16)
        values = v_ref[rows, :]
        cum[rows, :] = column
        end = column[BLOCK - 1 : BLOCK, :]
        ends.append(end)
        scaled = rk[rows].astype(F32) * jnp.exp(end - column)
        high, low = parts_of(scaled, 2)
        upd[b] = mm(high, values, 0, 0) + mm(low, values, 0, 0)
        ins[rows, :] = mm(weights, values)
    whole = jnp.exp(ends[1]) * upd[0] + upd[1]
    total = ends[0] + ends[1]
    for s in range(Z):
        sts[s, 0:8, :] = whole[s * 8 : (s + 1) * 8, :]
        sts[s, 8:9, :] = total
    upd[1] = jnp.broadcast_to(jnp.exp(ends[0]), (BLOCK, W))

    owner = c == lax.rem(z, C)
    str_[e] = sts[z]

    def give(i, carry):
        s = lax.rem(z + i, Z)

        @pl.when(jnp.logical_or(i > 0, jnp.logical_not(owner)))
        def _():
            pltpu.make_async_remote_copy(
                src_ref=sts.at[s],
                dst_ref=str_.at[e],
                send_sem=zsem.at[4],
                recv_sem=zsem.at[5],
                device_id={"ep_0": s, "ep_1": lax.rem(s, C)},
                device_id_type=MESH,
            ).start()

        return carry

    def give_states():
        lax.fori_loop(0, Z, give, 0)

    place = (y, x)
    moe = []
    for n in range(CHUNKS):
        moe.append(
            Spread(
                rbuf, (n * CHUNK, n * CHUNK + CHUNK // 2), CHUNK // 2, place, RELAY_ROWS[n],
                send.at[1], lambda k, n=n: recv.at[3 + 4 * n + k],
            )
        )
    mix = Spread(ho, (0, BLOCK), BLOCK, place, RELAY_HEADS, send.at[2], lambda k: recv.at[31 + k])

    def rows_of(n):
        return slice(n * CHUNK, (n + 1) * CHUNK), pl.ds(n * CHUNK, CHUNK)

    def arrive(n):
        count = 7 if n == 0 else 8
        landed(rbuf.at[t, pl.ds(0, count * CAP)], zsem.at[8 + n])
        moe[n].own()

    def hidden(n):
        moe[n].rest()
        rows, at = rows_of(n)
        left = jnp.concatenate([rbuf[k, rows, :] for k in range(T)], axis=1)
        units = (silu(mm(left, wg[...])) * mm(left, wu[...])).astype(BF16)
        ha[x, rows, :] = units[:, 0:W]
        hb[y, rows, :] = units[:, W : 2 * W]
        def straight():
            for side in range(2):
                hop(n, side, 0, 2)

        chosen(RELAY_HIDDEN[n], None, straight)
        for to in (1, -1):
            for side in range(2):
                hop(n, side, 0, to)

    hsides = ((ha, "tp_1", x), (hb, "tp_0", y))

    def hop(n, side, block, to, part=None):
        buf, axis, me = hsides[side]
        at = pl.ds(n * CHUNK, CHUNK)
        if part is not None:
            at = pl.ds(n * CHUNK + part * CHUNK // 2, CHUNK // 2)
        ref = buf.at[lax.rem(me + block + 4, 4), at]
        near = block == 0 and to != 2
        pltpu.make_async_remote_copy(
            src_ref=ref, dst_ref=ref, send_sem=send.at[3],
            recv_sem=recv.at[19 + 2 * n + (0 if near else 1)],
            device_id={axis: lax.rem(me + to + 4, 4)}, device_id_type=MESH,
        ).start()

    def hop_relay(n):
        landed(rows_in(ha, 4 * CHUNK), recv.at[19 + 2 * n])

        def onward():
            for side in range(2):
                hop(n, side, -1, 1, 0)
                hop(n, side, 1, -1, 1)

        chosen(RELAY_HIDDEN[n], onward, None)

    def down(n):
        landed(rows_in(ha, 2 * CHUNK), recv.at[20 + 2 * n])
        rows, at = rows_of(n)
        for side in range(2):
            buf, weight, out, into, axis, me = (
                (ha, wa, pa, ra, "tp_0", y), (hb, wb, pb, rb, "tp_1", x),
            )[side]
            left = jnp.concatenate([buf[k, rows, :] for k in range(4)], axis=1)
            right = jnp.concatenate(
                [weight[lax.rem(me + s, 4)].reshape(4 * W, W) for s in range(4)], axis=1
            )
            whole = mm(left, right)
            for s in (2, 1, 3):
                out[s - 1, rows, :] = whole[:, s * W : (s + 1) * W].astype(BF16)
                pltpu.make_async_remote_copy(
                    src_ref=out.at[s - 1, at], dst_ref=into.at[s - 1, at],
                    send_sem=send.at[4], recv_sem=recv.at[27 + n],
                    device_id={axis: lax.rem(me + s, 4)}, device_id_type=MESH,
                ).start()
            psum[side, rows, :] = whole[:, 0:W]

    def give_back(d, slot):
        pltpu.make_async_remote_copy(
            src_ref=eo.at[tile(slot)],
            dst_ref=ret.at[mine_at],
            send_sem=zsem.at[2],
            recv_sem=zsem.at[3],
            device_id=ring_dev(E + d)[1],
            device_id_type=MESH,
        ).start()

    def finish(n):
        landed(ra.at[pl.ds(0, 3), pl.ds(0, 2 * CHUNK)], recv.at[27 + n])
        rows, _ = rows_of(n)
        summed = psum[0, rows, :] + psum[1, rows, :]
        for into in (ra, rb):
            for s in range(3):
                summed = summed + into[s, rows, :].astype(F32)
        eo[rows, :] = summed.astype(BF16)
        if n == 0:
            ret[mine_at, :] = eo[own_rows, :]
        each(n, give_back)

    def scan_states():
        @pl.when(owner)
        def _():
            landed(str_.at[pl.ds(0, E - 1)], zsem.at[5])
            current = jnp.zeros((8, W), F32)
            for j in range(E):
                sto[j] = current
                if j + 1 < E:
                    current = jnp.exp(str_[j, 8:9, :]) * current + str_[j, 0:8, :]
            sti[z] = sto[e]

            def back(i, _):
                j, dev = ring_dev(i + 1)
                pltpu.make_async_remote_copy(
                    src_ref=sto.at[j],
                    dst_ref=sti.at[z],
                    send_sem=zsem.at[6],
                    recv_sem=zsem.at[7],
                    device_id=dev,
                    device_id_type=MESH,
                ).start()
                return _

            lax.fori_loop(0, E - 1, back, 0)

    def retain():
        @pl.when(owner)
        def _():
            landed(sti.at[pl.ds(0, Z - 1)], zsem.at[7])

        @pl.when(jnp.logical_not(owner))
        def _():
            landed(sti, zsem.at[7])

        entering = sti[...].reshape(W, W)
        for b in range(2):
            rows = slice(b * BLOCK, (b + 1) * BLOCK)
            high, low = parts_of(entering, 2)
            query = rotq[rows, :]
            carried = (mm(query, high) + mm(query, low)) * jnp.exp(cum[rows, :])
            retained = ins[rows, :] + carried
            mean = jnp.sum(retained * retained, axis=-1, keepdims=True) * (1.0 / W)
            gate = g_ref[rows, :].astype(F32)
            ho[t, rows, :] = (retained * lax.rsqrt(mean + 1e-05) * silu(gate)).astype(BF16)
            entering = upd[1] * entering + upd[0]

    def weights_here(n):
        for copy in local[:2]:
            copy.wait()

    def down_weights_here(n):
        for copy in local[2:4]:
            copy.wait()
        landed(wa.at[pl.ds(0, 3)], recv.at[0])
        landed(wb.at[pl.ds(0, 3)], recv.at[1])

    steps = {
        "O": arrive,
        "F": lambda n: moe[n].first(),
        "L": lambda n: moe[n].relay(),
        "U": weights_here,
        "H": hidden,
        "K": hop_relay,
        "V": down_weights_here,
        "D": down,
        "X": finish,
        "W": lambda n: send_weights(2),
        "G": lambda n: give_states(),
        "S": lambda n: scan_states(),
        "R": lambda n: retain(),
        "M": lambda n: (mix.own, mix.first, mix.relay, mix.rest)[n](),
    }
    for name in ORDER:
        steps[name[0]](int(name[1]))
    local[4].wait()
    heads = jnp.concatenate([ho[k] for k in range(T)], axis=1)
    mix_ref[...] = mm(heads, wo[...]).astype(BF16)
    mix_out = pltpu.make_async_copy(mix_ref, out_hbm.at[0], lsem.at[0])
    mix_out.start()

    landed(ret.at[pl.ds(0, (E - 1) * CAP)], zsem.at[3])
    moe_out = jnp.zeros((ROWS, W), F32)
    for k in range(2):
        share = jnp.transpose(jnp.broadcast_to(rw_ref[k : k + 1, :], (W, ROWS)))
        moe_out = moe_out + mm(oh[k], ret[...], 0, 0) * share
    moe_ref[...] = moe_out.astype(BF16)
    moe_copy = pltpu.make_async_copy(moe_ref, out_hbm.at[1], lsem.at[1])
    moe_copy.start()

    for n, region in (
        (0, rbuf.at[pl.ds(0, 6)]), (1, rbuf.at[pl.ds(0, 15)]), (2, ho.at[pl.ds(0, 15)]),
        (3, rbuf.at[pl.ds(0, 6)]), (4, rbuf.at[pl.ds(0, 6)]),
    ):
        departed(region, send.at[n])
    departed(snd.at[pl.ds(0, (E - 1) * CAP)], zsem.at[0])
    departed(eo.at[pl.ds(0, (E - 1) * CAP)], zsem.at[2])

    @pl.when(owner)
    def _():
        departed(sts.at[pl.ds(0, Z - 1)], zsem.at[4])
        departed(sto.at[pl.ds(0, E - 1)], zsem.at[6])

    @pl.when(jnp.logical_not(owner))
    def _():
        departed(sts, zsem.at[4])

    mix_out.wait()
    moe_copy.wait()


def tables():
    half = W // 2
    inverse = 10000.0 ** (-np.arange(half, dtype=np.float64) / half)
    near = np.arange(ROWS, dtype=np.float64)[:, None] * inverse[None, :]
    base = (np.arange(E, dtype=np.float64) * ROWS)[:, None] * inverse[None, :]
    both_halves = lambda a: np.concatenate([a, a], axis=1).astype(np.float32)
    return (
        both_halves(np.cos(near)),
        both_halves(np.sin(near)),
        both_halves(np.cos(base))[:, None, :],
        both_halves(np.sin(base))[:, None, :],
    )


def on_device(
    queries, keys, values, gates, log_decay, out_weight,
    moe_rows, moe_gain, routes, route_weights, gate_proj, up_proj, down_proj,
):
    hbm = pl.BlockSpec(memory_space=pltpu.HBM)
    scratch = [
        pltpu.VMEM((ROWS, W), BF16),
        pltpu.VMEM((ROWS, W), BF16),
        pltpu.VMEM((ROWS, W), BF16),
        pltpu.VMEM((ROWS, W), BF16),
        pltpu.VMEM((2, BLOCK), F32),
        pltpu.VMEM((ROWS, D), BF16),
        pltpu.VMEM((T, W), BF16),
        pltpu.VMEM((2, ROWS), jnp.int32),
        pltpu.VMEM((2, ROWS), F32),
        pltpu.VMEM((ROWS, W), F32),
        pltpu.VMEM((ROWS, W), F32),
        pltpu.VMEM((1, W), F32),
        pltpu.VMEM((1, W), F32),
        pltpu.VMEM((ROWS, W), BF16),
        pltpu.VMEM((ROWS, W), BF16),
        pltpu.VMEM((D, 256), BF16),
        pltpu.VMEM((D, 256), BF16),
        pltpu.VMEM((D, W), BF16),
        pltpu.VMEM((Y, X, W, W), BF16),
        pltpu.VMEM((X, Y, W, W), BF16),
        pltpu.VMEM((2, SLOTS, ROWS), BF16),
        pltpu.VMEM((SLOTS, W), BF16),
        pltpu.VMEM((T, SLOTS, W), BF16),
        pltpu.VMEM((X, SLOTS, W), BF16),
        pltpu.VMEM((Y, SLOTS, W), BF16),
        pltpu.VMEM((3, SLOTS, W), BF16),
        pltpu.VMEM((3, SLOTS, W), BF16),
        pltpu.VMEM((3, SLOTS, W), BF16),
        pltpu.VMEM((3, SLOTS, W), BF16),
        pltpu.VMEM((SLOTS, W), BF16),
        pltpu.VMEM((SLOTS, W), BF16),
        pltpu.VMEM((Z, 9, W), F32),
        pltpu.VMEM((E, 9, W), F32),
        pltpu.VMEM((E, 8, W), F32),
        pltpu.VMEM((Z, 8, W), F32),
        pltpu.VMEM((ROWS, W), F32),
        pltpu.VMEM((ROWS, W), BF16),
        pltpu.VMEM((ROWS, W), F32),
        pltpu.VMEM((2, W, W), F32),
        pltpu.VMEM((T, ROWS, W), BF16),
        pltpu.VMEM((2, SLOTS, W), F32),
        pltpu.SemaphoreType.DMA((18,)),
        pltpu.SemaphoreType.DMA((5,)),
        pltpu.SemaphoreType.DMA((35,)),
        pltpu.SemaphoreType.DMA((12,)),
    ]
    out = jax.ShapeDtypeStruct((2, ROWS, W), BF16)
    found = pl.pallas_call(
        kernel,
        out_shape=out,
        in_specs=[hbm] * 17,
        out_specs=hbm,
        scratch_shapes=scratch,
        compiler_params=pltpu.CompilerParams(
            collective_id=0, has_side_effects=True, vmem_limit_bytes=67043328
        ),
    )(
        queries, keys, values, gates, log_decay.reshape(2, BLOCK), out_weight,
        moe_rows, moe_gain.reshape(T, W), routes.T, route_weights.T,
        gate_proj.reshape(D, 256), up_proj.reshape(D, 256),
        down_proj.reshape(Y, X, 2, W, W), *tables(),
    )
    return found[0], found[1]


def solution(mesh):
    torus = Mesh(mesh.devices.reshape(Z, C, Y, X), ("ep_0", "ep_1", "tp_0", "tp_1"))
    return jax.shard_map(
        on_device,
        mesh=torus,
        in_specs=(
            P(EP, TP), P(EP, TP), P(EP, TP), P(EP, TP), P(EP, TP), P(None, TP),
            P(EP, None), P(), P(EP, None), P(EP, None),
            P(EP, None, TP), P(EP, None, TP), P(EP, None, TP),
        ),
        out_specs=(P(EP, TP), P(EP, TP)),
        check_vma=False,
    )
```

```python
import jax
import jax.numpy as jnp
import numpy as np
from jax import lax
from jax.experimental import pallas as pl
from jax.experimental.pallas import tpu as pltpu
from jax.sharding import Mesh
from jax.sharding import PartitionSpec as P

MESH = pl.DeviceIdType.MESH
F32 = jnp.float32
BF16 = jnp.bfloat16
Z, C, Y, X = 16, 2, 4, 4
E = Z * C
T = Y * X
ROWS = 256
SLOTS = 2 * ROWS
CAP = SLOTS // E
D = 2048
W = 128
BLOCK = 128
CHUNKS = 4
ORDER = (
    "W0", "O0", "O3", "G0", "F0", "O1", "O2", "F3", "F1", "F2", "L0", "S0", "L3", "L1", "L2",
    "U0", "H0", "H1", "H2", "H3", "R0", "M0", "V0", "K1", "D1", "K2", "D2", "K0", "D0", "K3",
    "D3", "X1", "M1", "X2", "X0", "X3", "M2", "M3",
)
RELAY_ROWS = (1, 1, 1, 1)
RELAY_HIDDEN = (0, 0, 0, 0)
RELAY_HEADS = 1
CHUNK = SLOTS // CHUNKS
OWN = 4
EP = ("ep_0", "ep_1")
TP = ("tp_0", "tp_1")


def mm(a, b, ca=1, cb=0):
    return lax.dot_general(a, b, (((ca,), (cb,)), ((), ())), preferred_element_type=F32)


def parts_of(a, count):
    found = []
    for k in range(count):
        piece = a.astype(BF16)
        found.append(piece)
        if k + 1 < count:
            a = a - piece.astype(F32)
    return found


def silu(v):
    return v / (1.0 + jnp.exp(-v))


def chosen(relayed, onward, straight):
    act = (straight, onward)
    if relayed < 2:
        if act[relayed] is not None:
            act[relayed]()
        return
    for core in range(2):
        if act[core] is not None:
            pl.when(lax.axis_index("ep_1") == core)(act[core])


def rows_in(buf, rows):
    count = 1
    while rows % count or rows // count > buf.shape[1]:
        count += 1
    return buf.at[pl.ds(0, count), pl.ds(0, rows // count)]


class Spread:
    def __init__(self, buf, starts, n, place, relayed, send, recv):
        self.buf, self.starts, self.n, self.place = buf, starts, n, place
        self.relayed, self.send, self.recv = relayed, send, recv

    def block(self, half, dp, dq):
        y, x = self.place
        dy, dx = (dq, dp) if half == 0 else (dp, dq)
        return lax.rem(y + dy + Y, Y), lax.rem(x + dx + X, X)

    def go(self, half, k, frm, to, part=None):
        y, x = self.block(half, *frm)
        start, count = self.starts[half], self.n
        if part is not None:
            count //= 2
            start += part * count
        ref = self.buf.at[y * X + x, pl.ds(start, count)]
        ty, tx = self.block(half, *to)
        pltpu.make_async_remote_copy(
            src_ref=ref,
            dst_ref=ref,
            send_sem=self.send,
            recv_sem=self.recv(k),
            device_id={"tp_0": ty, "tp_1": tx},
            device_id_type=MESH,
        ).start()

    def across(self, j):
        def straight():
            for half in range(2):
                self.go(half, 3, (j, 0), (0, 2))

        chosen(self.relayed, None, straight)
        for to in (1, -1):
            for half in range(2):
                self.go(half, 2 if j else 1, (j, 0), (0, to))

    def own(self):
        for to in (2, -1, 1):
            for half in range(2):
                self.go(half, 0, (0, 0), (to, 0))
        self.across(0)

    def first(self):
        self.got(0, 6)
        for j in (-1, 1, 2):
            self.across(j)

    def relay(self):
        for k, blocks, js in ((1, 4, (0,)), (2, 12, (-1, 1, 2))):
            self.got(k, blocks)

            def onward(js=js):
                for j in js:
                    for half in range(2):
                        self.go(half, 3, (j, -1), (0, 1), 0)
                        self.go(half, 3, (j, 1), (0, -1), 1)

            chosen(self.relayed, onward, None)

    def rest(self):
        self.got(3, 8)

    def got(self, k, blocks):
        landed(rows_in(self.buf, blocks * self.n), self.recv(k))


def whole_copy(region, sem):
    return pltpu.make_async_remote_copy(
        src_ref=region,
        dst_ref=region,
        send_sem=sem,
        recv_sem=sem,
        device_id={"tp_1": lax.rem(lax.axis_index("tp_1") + 1, X)},
        device_id_type=MESH,
    )


def landed(region, sem):
    whole_copy(region, sem).wait_recv()


def departed(region, sem):
    whole_copy(region, sem).wait_send()


def kernel(
    q_hbm, k_hbm, v_hbm, g_hbm, ld_hbm, wo_hbm, rows_hbm, gain_hbm, routes_hbm, rw_hbm,
    wg_hbm, wu_hbm, wd_hbm, cr_hbm, sr_hbm, cb_hbm, sb_hbm,
    out_hbm,
    q_ref, k_ref, v_ref, g_ref, ld_ref, rows_ref, gain_ref, routes_ref, rw_ref,
    cr_ref, sr_ref, cb_ref, sb_ref, mix_ref, moe_ref,
    wg, wu, wo, wa, wb, oh, snd, rbuf, ha, hb, pa, pb, ra, rb, eo, ret,
    sts, str_, sto, sti, ins, rotq, cum, upd, ho, psum, oht, share,
    lsem, send, recv, zsem,
):
    z, c = lax.axis_index("ep_0"), lax.axis_index("ep_1")
    y, x = lax.axis_index("tp_0"), lax.axis_index("tp_1")
    e = z * C + c
    t = y * X + x

    barrier = pltpu.get_barrier_semaphore()

    def ring_dev(d):
        j = lax.rem(e + d, E)
        return j, {"ep_0": j // C, "ep_1": lax.rem(j, C)}

    wd_rows = wd_hbm
    routed = (
        (routes_hbm, routes_ref), (rows_hbm, rows_ref), (gain_hbm, gain_ref), (rw_hbm, rw_ref),
    )
    mixed = (
        (k_hbm, k_ref), (q_hbm, q_ref), (v_hbm, v_ref), (ld_hbm, ld_ref), (cr_hbm, cr_ref),
        (sr_hbm, sr_ref), (cb_hbm.at[e], cb_ref), (sb_hbm.at[e], sb_ref), (g_hbm, g_ref),
    )
    held = (
        (wg_hbm, wg), (wu_hbm, wu), (wd_rows.at[y, :, 0], wa.at[y]),
        (wd_rows.at[:, x, 1], wb.at[x]), (wo_hbm, wo),
    )
    local = [
        pltpu.make_async_copy(src, dst, lsem.at[n])
        for n, (src, dst) in enumerate(routed + mixed + held)
    ]
    routed, mixed, local = (
        local[: len(routed)], local[len(routed) : -len(held)], local[-len(held) :],
    )
    for copy in routed:
        copy.start()

    def greet(d):
        pl.semaphore_signal(barrier, inc=1, device_id=ring_dev(d)[1], device_id_type=MESH)

    for d in sorted(range(1, E), key=lambda d: -min(d, E - d)):
        greet(d)
    for s in range(1, 4):
        pl.semaphore_signal(
            barrier, inc=1, device_id={"tp_0": lax.rem(y + s, Y)}, device_id_type=MESH
        )
        pl.semaphore_signal(
            barrier, inc=1, device_id={"tp_1": lax.rem(x + s, X)}, device_id_type=MESH
        )

    for copy in mixed + local:
        copy.start()

    for copy in routed:
        copy.wait()

    slot_id = lax.broadcasted_iota(jnp.int32, (SLOTS, ROWS), 0)
    expert_of = slot_id // CAP
    place_of = (slot_id - expert_of * CAP).astype(F32)
    named = [routes_ref[k : k + 1, :] == expert_of for k in range(2)]
    either = jnp.logical_or(named[0], named[1])
    before = (
        lax.broadcasted_iota(jnp.int32, (ROWS, ROWS), 0)
        < lax.broadcasted_iota(jnp.int32, (ROWS, ROWS), 1)
    )
    rank = mm(either.astype(F32).astype(BF16), before.astype(F32).astype(BF16))
    here = rank == place_of
    for k in range(2):
        oh[k] = jnp.logical_and(named[k], here).astype(F32).astype(BF16)

    lanes = pl.ds(pl.multiple_of(t * W, W), W)
    gain_at = lax.broadcasted_iota(jnp.int32, (T, W), 0) == t
    gain = jnp.sum(jnp.where(gain_at, gain_ref[...].astype(F32), 0.0), axis=0, keepdims=True)

    def squares(r, _):
        rows = pl.ds(pl.multiple_of(r * 64, 64), 64)
        full = rows_ref[rows, :].astype(F32)
        mean = jnp.sum(full * full, axis=-1, keepdims=True) * (1.0 / D)
        mine = rows_ref[rows, lanes].astype(F32)
        normed = mine * lax.rsqrt(mean + 1e-06) * gain
        rotq[rows, :] = normed.astype(BF16)
        return _

    lax.fori_loop(0, ROWS // 64, squares, 0)
    normed = rotq[...]
    picked = mm(oh[0] + oh[1], normed)
    snd[...] = picked.astype(BF16)
    mine_at = pl.ds(pl.multiple_of(e * CAP, CAP), CAP)
    own_rows = slice(OWN * CAP, (OWN + 1) * CAP)
    rbuf[t, own_rows, :] = snd[mine_at, :]

    pl.semaphore_wait(barrier, E - 1 + 6)

    def zigzag(i, low, high):
        even = 1 - lax.rem(i, 2)
        return even * (low + i // 2) + (1 - even) * (high - i // 2)

    def source_of(n, i):
        if n == 0:
            d = zigzag(i, -4, 3)
            return d, OWN + d
        if n == 1:
            return 15 - i, 15 - i
        if n == 2:
            return 16 + i, 16 + i
        d = zigzag(i, -8, 7)
        even = 1 - lax.rem(i, 2)
        return d, 20 + d + 16 * even

    def tile(k):
        return pl.ds(pl.multiple_of(k * CAP, CAP), CAP)

    def each(n, act):
        def step(i, carry):
            act(*source_of(n, i))
            return carry

        lax.fori_loop(0, 7 if n == 0 else 8, step, 0)

    for n in (0, 3, 1, 2):

        def dispatch(d, slot, n=n):
            j, dev = ring_dev(E - d)
            pltpu.make_async_remote_copy(
                src_ref=snd.at[tile(j)],
                dst_ref=rbuf.at[t, tile(slot)],
                send_sem=zsem.at[0],
                recv_sem=zsem.at[8 + n],
                device_id=dev,
                device_id_type=MESH,
            ).start()

        each(n, dispatch)

    def weight_copy(src, dst, sem, axis, to):
        me = y if axis == "tp_0" else x
        pltpu.make_async_remote_copy(
            src_ref=src, dst_ref=dst, send_sem=send.at[0], recv_sem=recv.at[sem],
            device_id={axis: lax.rem(me + to + 4, 4)}, device_id_type=MESH,
        ).start()

    wsides = ((wa, "tp_0", y), (wb, "tp_1", x))

    def send_weights(*shifts):
        for side, (into, axis, me) in enumerate(wsides):
            for to in shifts:
                k = lax.rem(me + to + 4, 4)
                rows = wd_rows.at[k, :, 0] if side == 0 else wd_rows.at[:, k, 1]
                weight_copy(rows, into.at[me], side, axis, to)

    send_weights(1, -1)

    for copy in mixed:
        copy.wait()
    cb, sb = cb_ref[...], sb_ref[...]
    cos = cb * cr_ref[...] - sb * sr_ref[...]

    def signed(first, second):
        lane = lax.broadcasted_iota(jnp.int32, first.shape, 1)
        return jnp.where(lane < W // 2, -first, second)

    sin = sb * cr_ref[...] + cb * sr_ref[...]
    sin = signed(sin, sin)

    def turned(ref):
        full = ref[...].astype(F32)
        return full * cos + pltpu.roll(full, W // 2, 1) * sin

    rq = turned(q_ref).astype(BF16)
    rotq[...] = rq
    rk = (turned(k_ref) * (W**-0.5)).astype(BF16)
    row_i = lax.broadcasted_iota(jnp.int32, (BLOCK, BLOCK), 0)
    col_i = lax.broadcasted_iota(jnp.int32, (BLOCK, BLOCK), 1)
    causal = row_i >= col_i
    tri = causal.astype(F32).astype(BF16)
    ends = []
    for b in range(2):
        rows = slice(b * BLOCK, (b + 1) * BLOCK)
        decay = jnp.broadcast_to(ld_ref[b : b + 1, :], (BLOCK, BLOCK))
        column = jnp.zeros((BLOCK, BLOCK), F32)
        line = jnp.zeros((BLOCK, BLOCK), F32)
        for piece in parts_of(decay, 3):
            column = column + mm(tri, piece, 1, 1)
            line = line + mm(piece, tri, 1, 1)
        spread = column - line
        factor = jnp.where(causal, jnp.exp(jnp.where(causal, spread, 0.0)), 0.0)
        weights = (mm(rq[rows], rk[rows], 1, 1) * factor).astype(BF16)
        values = v_ref[rows, :]
        cum[rows, :] = column
        end = column[BLOCK - 1 : BLOCK, :]
        ends.append(end)
        scaled = rk[rows].astype(F32) * jnp.exp(end - column)
        high, low = parts_of(scaled, 2)
        upd[b] = mm(high, values, 0, 0) + mm(low, values, 0, 0)
        ins[rows, :] = mm(weights, values)
    whole = jnp.exp(ends[1]) * upd[0] + upd[1]
    total = ends[0] + ends[1]
    for s in range(Z):
        sts[s, 0:8, :] = whole[s * 8 : (s + 1) * 8, :]
        sts[s, 8:9, :] = total
    upd[1] = jnp.broadcast_to(jnp.exp(ends[0]), (BLOCK, W))

    owner = c == lax.rem(z, C)
    str_[e] = sts[z]

    def give(i, carry):
        s = lax.rem(z + i, Z)

        @pl.when(jnp.logical_or(i > 0, jnp.logical_not(owner)))
        def _():
            pltpu.make_async_remote_copy(
                src_ref=sts.at[s],
                dst_ref=str_.at[e],
                send_sem=zsem.at[4],
                recv_sem=zsem.at[5],
                device_id={"ep_0": s, "ep_1": lax.rem(s, C)},
                device_id_type=MESH,
            ).start()

        return carry

    def give_states():
        lax.fori_loop(0, Z, give, 0)

    place = (y, x)
    moe = []
    for n in range(CHUNKS):
        moe.append(
            Spread(
                rbuf, (n * CHUNK, n * CHUNK + CHUNK // 2), CHUNK // 2, place, RELAY_ROWS[n],
                send.at[1], lambda k, n=n: recv.at[3 + 4 * n + k],
            )
        )
    mix = Spread(ho, (0, BLOCK), BLOCK, place, RELAY_HEADS, send.at[2], lambda k: recv.at[31 + k])

    def rows_of(n):
        return slice(n * CHUNK, (n + 1) * CHUNK), pl.ds(n * CHUNK, CHUNK)

    def arrive(n):
        count = 7 if n == 0 else 8
        landed(rbuf.at[t, pl.ds(0, count * CAP)], zsem.at[8 + n])
        moe[n].own()

    def hidden(n):
        moe[n].rest()
        rows, at = rows_of(n)
        left = jnp.concatenate([rbuf[k, rows, :] for k in range(T)], axis=1)
        units = (silu(mm(left, wg[...])) * mm(left, wu[...])).astype(BF16)
        ha[x, rows, :] = units[:, 0:W]
        hb[y, rows, :] = units[:, W : 2 * W]
        def straight():
            for side in range(2):
                hop(n, side, 0, 2)

        chosen(RELAY_HIDDEN[n], None, straight)
        for to in (1, -1):
            for side in range(2):
                hop(n, side, 0, to)

    hsides = ((ha, "tp_1", x), (hb, "tp_0", y))

    def hop(n, side, block, to, part=None):
        buf, axis, me = hsides[side]
        at = pl.ds(n * CHUNK, CHUNK)
        if part is not None:
            at = pl.ds(n * CHUNK + part * CHUNK // 2, CHUNK // 2)
        ref = buf.at[lax.rem(me + block + 4, 4), at]
        near = block == 0 and to != 2
        pltpu.make_async_remote_copy(
            src_ref=ref, dst_ref=ref, send_sem=send.at[3],
            recv_sem=recv.at[19 + 2 * n + (0 if near else 1)],
            device_id={axis: lax.rem(me + to + 4, 4)}, device_id_type=MESH,
        ).start()

    def hop_relay(n):
        landed(rows_in(ha, 4 * CHUNK), recv.at[19 + 2 * n])

        def onward():
            for side in range(2):
                hop(n, side, -1, 1, 0)
                hop(n, side, 1, -1, 1)

        chosen(RELAY_HIDDEN[n], onward, None)

    def down(n):
        landed(rows_in(ha, 2 * CHUNK), recv.at[20 + 2 * n])
        rows, at = rows_of(n)
        for side in range(2):
            buf, weight, out, into, axis, me = (
                (ha, wa, pa, ra, "tp_0", y), (hb, wb, pb, rb, "tp_1", x),
            )[side]
            left = jnp.concatenate([buf[k, rows, :] for k in range(4)], axis=1)
            right = jnp.concatenate(
                [weight[lax.rem(me + s, 4)].reshape(4 * W, W) for s in range(4)], axis=1
            )
            whole = mm(left, right)
            for s in (2, 1, 3):
                out[s - 1, rows, :] = whole[:, s * W : (s + 1) * W].astype(BF16)
                pltpu.make_async_remote_copy(
                    src_ref=out.at[s - 1, at], dst_ref=into.at[s - 1, at],
                    send_sem=send.at[4], recv_sem=recv.at[27 + n],
                    device_id={axis: lax.rem(me + s, 4)}, device_id_type=MESH,
                ).start()
            psum[side, rows, :] = whole[:, 0:W]

    def give_back(d, slot):
        pltpu.make_async_remote_copy(
            src_ref=eo.at[tile(slot)],
            dst_ref=ret.at[mine_at],
            send_sem=zsem.at[2],
            recv_sem=zsem.at[3],
            device_id=ring_dev(E + d)[1],
            device_id_type=MESH,
        ).start()

    def finish(n):
        landed(ra.at[pl.ds(0, 3), pl.ds(0, 2 * CHUNK)], recv.at[27 + n])
        rows, _ = rows_of(n)
        summed = psum[0, rows, :] + psum[1, rows, :]
        for into in (ra, rb):
            for s in range(3):
                summed = summed + into[s, rows, :].astype(F32)
        eo[rows, :] = summed.astype(BF16)
        if n == 0:
            ret[mine_at, :] = eo[own_rows, :]
        each(n, give_back)

    def scan_states():
        @pl.when(owner)
        def _():
            landed(str_.at[pl.ds(0, E - 1)], zsem.at[5])
            current = jnp.zeros((8, W), F32)
            for j in range(E):
                sto[j] = current
                if j + 1 < E:
                    current = jnp.exp(str_[j, 8:9, :]) * current + str_[j, 0:8, :]
            sti[z] = sto[e]

            def back(i, _):
                j, dev = ring_dev(i + 1)
                pltpu.make_async_remote_copy(
                    src_ref=sto.at[j],
                    dst_ref=sti.at[z],
                    send_sem=zsem.at[6],
                    recv_sem=zsem.at[7],
                    device_id=dev,
                    device_id_type=MESH,
                ).start()
                return _

            lax.fori_loop(0, E - 1, back, 0)

    def retain():
        @pl.when(owner)
        def _():
            landed(sti.at[pl.ds(0, Z - 1)], zsem.at[7])

        @pl.when(jnp.logical_not(owner))
        def _():
            landed(sti, zsem.at[7])

        entering = sti[...].reshape(W, W)
        for b in range(2):
            rows = slice(b * BLOCK, (b + 1) * BLOCK)
            high, low = parts_of(entering, 2)
            query = rotq[rows, :]
            carried = (mm(query, high) + mm(query, low)) * jnp.exp(cum[rows, :])
            retained = ins[rows, :] + carried
            mean = jnp.sum(retained * retained, axis=-1, keepdims=True) * (1.0 / W)
            gate = g_ref[rows, :].astype(F32)
            ho[t, rows, :] = (retained * lax.rsqrt(mean + 1e-05) * silu(gate)).astype(BF16)
            entering = upd[1] * entering + upd[0]

    def weights_here(n):
        for copy in local[:2]:
            copy.wait()

    def down_weights_here(n):
        for copy in local[2:4]:
            copy.wait()
        landed(wa.at[pl.ds(0, 3)], recv.at[0])
        landed(wb.at[pl.ds(0, 3)], recv.at[1])

    steps = {
        "O": arrive,
        "F": lambda n: moe[n].first(),
        "L": lambda n: moe[n].relay(),
        "U": weights_here,
        "H": hidden,
        "K": hop_relay,
        "V": down_weights_here,
        "D": down,
        "X": finish,
        "W": lambda n: send_weights(2),
        "G": lambda n: give_states(),
        "S": lambda n: scan_states(),
        "R": lambda n: retain(),
        "M": lambda n: (mix.own, mix.first, mix.relay, mix.rest)[n](),
    }
    for k in range(2):
        oht[k] = jnp.transpose(oh[k].astype(F32)).astype(BF16)
        share[k] = jnp.transpose(jnp.broadcast_to(rw_ref[k : k + 1, :], (W, ROWS)))

    for name in ORDER:
        steps[name[0]](int(name[1]))
    local[4].wait()
    heads = jnp.concatenate([ho[k] for k in range(T)], axis=1)
    mix_ref[...] = mm(heads, wo[...]).astype(BF16)
    mix_out = pltpu.make_async_copy(mix_ref, out_hbm.at[0], lsem.at[0])
    mix_out.start()

    landed(ret.at[pl.ds(0, (E - 1) * CAP)], zsem.at[3])
    moe_out = jnp.zeros((ROWS, W), F32)
    for k in range(2):
        moe_out = moe_out + mm(oht[k], ret[...]) * share[k]
    moe_ref[...] = moe_out.astype(BF16)
    moe_copy = pltpu.make_async_copy(moe_ref, out_hbm.at[1], lsem.at[1])
    moe_copy.start()

    for n, region in (
        (0, rbuf.at[pl.ds(0, 6)]), (1, rbuf.at[pl.ds(0, 15)]), (2, ho.at[pl.ds(0, 15)]),
        (3, rbuf.at[pl.ds(0, 6)]), (4, rbuf.at[pl.ds(0, 6)]),
    ):
        departed(region, send.at[n])
    departed(snd.at[pl.ds(0, (E - 1) * CAP)], zsem.at[0])
    departed(eo.at[pl.ds(0, (E - 1) * CAP)], zsem.at[2])

    @pl.when(owner)
    def _():
        departed(sts.at[pl.ds(0, Z - 1)], zsem.at[4])
        departed(sto.at[pl.ds(0, E - 1)], zsem.at[6])

    @pl.when(jnp.logical_not(owner))
    def _():
        departed(sts, zsem.at[4])

    mix_out.wait()
    moe_copy.wait()


def tables():
    half = W // 2
    inverse = 10000.0 ** (-np.arange(half, dtype=np.float64) / half)
    near = np.arange(ROWS, dtype=np.float64)[:, None] * inverse[None, :]
    base = (np.arange(E, dtype=np.float64) * ROWS)[:, None] * inverse[None, :]
    both_halves = lambda a: np.concatenate([a, a], axis=1).astype(np.float32)
    return (
        both_halves(np.cos(near)),
        both_halves(np.sin(near)),
        both_halves(np.cos(base))[:, None, :],
        both_halves(np.sin(base))[:, None, :],
    )


def on_device(
    queries, keys, values, gates, log_decay, out_weight,
    moe_rows, moe_gain, routes, route_weights, gate_proj, up_proj, down_proj,
):
    hbm = pl.BlockSpec(memory_space=pltpu.HBM)
    scratch = [
        pltpu.VMEM((ROWS, W), BF16),
        pltpu.VMEM((ROWS, W), BF16),
        pltpu.VMEM((ROWS, W), BF16),
        pltpu.VMEM((ROWS, W), BF16),
        pltpu.VMEM((2, BLOCK), F32),
        pltpu.VMEM((ROWS, D), BF16),
        pltpu.VMEM((T, W), BF16),
        pltpu.VMEM((2, ROWS), jnp.int32),
        pltpu.VMEM((2, ROWS), F32),
        pltpu.VMEM((ROWS, W), F32),
        pltpu.VMEM((ROWS, W), F32),
        pltpu.VMEM((1, W), F32),
        pltpu.VMEM((1, W), F32),
        pltpu.VMEM((ROWS, W), BF16),
        pltpu.VMEM((ROWS, W), BF16),
        pltpu.VMEM((D, 256), BF16),
        pltpu.VMEM((D, 256), BF16),
        pltpu.VMEM((D, W), BF16),
        pltpu.VMEM((Y, X, W, W), BF16),
        pltpu.VMEM((X, Y, W, W), BF16),
        pltpu.VMEM((2, SLOTS, ROWS), BF16),
        pltpu.VMEM((SLOTS, W), BF16),
        pltpu.VMEM((T, SLOTS, W), BF16),
        pltpu.VMEM((X, SLOTS, W), BF16),
        pltpu.VMEM((Y, SLOTS, W), BF16),
        pltpu.VMEM((3, SLOTS, W), BF16),
        pltpu.VMEM((3, SLOTS, W), BF16),
        pltpu.VMEM((3, SLOTS, W), BF16),
        pltpu.VMEM((3, SLOTS, W), BF16),
        pltpu.VMEM((SLOTS, W), BF16),
        pltpu.VMEM((SLOTS, W), BF16),
        pltpu.VMEM((Z, 9, W), F32),
        pltpu.VMEM((E, 9, W), F32),
        pltpu.VMEM((E, 8, W), F32),
        pltpu.VMEM((Z, 8, W), F32),
        pltpu.VMEM((ROWS, W), F32),
        pltpu.VMEM((ROWS, W), BF16),
        pltpu.VMEM((ROWS, W), F32),
        pltpu.VMEM((2, W, W), F32),
        pltpu.VMEM((T, ROWS, W), BF16),
        pltpu.VMEM((2, SLOTS, W), F32),
        pltpu.VMEM((2, ROWS, SLOTS), BF16),
        pltpu.VMEM((2, ROWS, W), F32),
        pltpu.SemaphoreType.DMA((18,)),
        pltpu.SemaphoreType.DMA((5,)),
        pltpu.SemaphoreType.DMA((35,)),
        pltpu.SemaphoreType.DMA((12,)),
    ]
    out = jax.ShapeDtypeStruct((2, ROWS, W), BF16)
    found = pl.pallas_call(
        kernel,
        out_shape=out,
        in_specs=[hbm] * 17,
        out_specs=hbm,
        scratch_shapes=scratch,
        compiler_params=pltpu.CompilerParams(
            collective_id=0, has_side_effects=True, vmem_limit_bytes=67043328
        ),
    )(
        queries, keys, values, gates, log_decay.reshape(2, BLOCK), out_weight,
        moe_rows, moe_gain.reshape(T, W), routes.T, route_weights.T,
        gate_proj.reshape(D, 256), up_proj.reshape(D, 256),
        down_proj.reshape(Y, X, 2, W, W), *tables(),
    )
    return found[0], found[1]


def solution(mesh):
    torus = Mesh(mesh.devices.reshape(Z, C, Y, X), ("ep_0", "ep_1", "tp_0", "tp_1"))
    return jax.shard_map(
        on_device,
        mesh=torus,
        in_specs=(
            P(EP, TP), P(EP, TP), P(EP, TP), P(EP, TP), P(EP, TP), P(None, TP),
            P(EP, None), P(), P(EP, None), P(EP, None),
            P(EP, None, TP), P(EP, None, TP), P(EP, None, TP),
        ),
        out_specs=(P(EP, TP), P(EP, TP)),
        check_vma=False,
    )
```
